512 devices in a mesh: ep: 32 (over z, core), tp: 16 (over y, x).
Axes of the slice: x: 4, y: 4, z: 16, core: 2. Of those that a mesh axis runs over, the one named last changes fastest.
Arguments:
- tokens: bfloat16 [512, 2048], P('ep'), may hold values from -6 to 6
- attn_gain: float32 [2048], replicated, may hold values from 0.1 to 1.9
- query_weight: bfloat16 [2048, 2048], P('ep', 'tp'), may hold values from -0.125 to 0.125
- key_weight: bfloat16 [2048, 2048], P('ep', 'tp'), may hold values from -0.125 to 0.125
- value_weight: bfloat16 [2048, 2048], P('ep', 'tp'), may hold values from -0.125 to 0.125
- forget_weight: bfloat16 [2048, 16], P(None, 'tp'), may hold values from -0.125 to 0.125
- forget_bias: float32 [16], P('tp'), may hold values from -1 to 2
- cache_keys: bfloat16 [512, 16, 384, 128], P('ep', 'tp'), may hold values from -240 to 240
- cache_values: bfloat16 [512, 16, 384, 128], P('ep', 'tp'), may hold values from -6 to 6
- cache_gates: float32 [512, 16, 384], P('ep', 'tp'), may hold values from -768 to 0, as said below
- lengths: int32 [512], P('ep'), may hold values from 1 to 384
- output_weight: bfloat16 [2048, 2048], P('tp', 'ep'), may hold values from -0.125 to 0.125
- ffn_gain: float32 [2048], replicated, may hold values from 0.1 to 1.9
- dense_gate_proj: bfloat16 [2048, 2048], P('ep', 'tp'), may hold values from -0.125 to 0.125
- dense_up_proj: bfloat16 [2048, 2048], P('ep', 'tp'), may hold values from -0.125 to 0.125
- dense_down_proj: bfloat16 [2048, 2048], P('tp', 'ep'), may hold values from -0.125 to 0.125
- dense_mix: bfloat16 [2048], replicated, may hold values from -0.125 to 0.125
- expert_ids: int32 [512, 2], P('ep'), may hold values from 0 to 31, as said below
- group_prob: float32 [512], P('ep'), may hold values from 0.25 to 1
- pair_prob: float32 [512, 2], P('ep'), may hold values from 0.05 to 1
- expert_gate: bfloat16 [32, 2048, 2048], P('ep', None, 'tp'), may hold values from -0.125 to 0.125
- expert_up: bfloat16 [32, 2048, 2048], P('ep', None, 'tp'), may hold values from -0.125 to 0.125
- expert_down: bfloat16 [32, 2048, 2048], P('ep', 'tp'), may hold values from -0.125 to 0.125
Outputs:
- mixed_out: bfloat16 [512, 2048], P('ep')
The draws below stay inside these ranges and needn't reach their ends.
Inputs may be any that keep to these rules, and one draw needn't show every extreme that they name: `expert_ids`: each row names two different experts of one group, the groups being 4 runs of consecutive ids. In each aligned block of 16 rows (the rows of one index of ep) no expert is named more than 2 times, and some expert exactly 2 times. `cache_gates`: along positions the values never rise.
All inputs are finite; a program needn't handle non-finite values.
Results may differ from the reference program's by a relative error of at most 0.014.
Values may be sent and summed in bfloat16 or wider, within the bound.
No kernel may reach another device: no remote copies, remote signals or barrier semaphores. Data moves between devices by JAX's collectives and lax.ppermute only.
A program may use at most 64 MiB of HBM per device.

```python
import math
import jax
import jax.numpy as jnp
from jax import lax

D = 2048
HEAD_TOTAL = 16
HEAD = 128
FF_D = 2048
FF_E = 2048
GROUPS = 4
SEQ_DEV = 16
CACHED_LENGTH = 384
SEQUENCE_TOTAL = 512
EXPERTS = 32
CAP = 2
N_EP = 32


def draw_cache_keys(key, part):
    first_key = jax.random.fold_in(key, 0)
    base = jnp.clip(jax.random.normal(first_key, (SEQUENCE_TOTAL, HEAD_TOTAL, CACHED_LENGTH, HEAD), jnp.float32), -6.0, 6.0)
    return base.astype(jnp.bfloat16)


def draw_cache_gates(key, part):
    every_key = jax.random.split(key, 7)
    fast_share = 0.5
    fast_heads = jax.random.uniform(every_key[0], (1, HEAD_TOTAL, 1), jnp.float32) < fast_share
    slow_rate = jnp.exp(jax.random.uniform(every_key[1], (SEQUENCE_TOTAL, HEAD_TOTAL, 1), jnp.float32, math.log(0.3), math.log(2.0))) / CACHED_LENGTH
    fast_rate = jnp.exp(jax.random.uniform(every_key[2], (SEQUENCE_TOTAL, HEAD_TOTAL, 1), jnp.float32, math.log(1.0 / 100.0), math.log(1.0 / 30.0)))
    seq_factor = jnp.exp(jax.random.uniform(every_key[3], (SEQUENCE_TOTAL, 1, 1), jnp.float32, math.log(0.5), math.log(2.0)))
    coarse_scores = jax.random.uniform(every_key[4], (SEQUENCE_TOTAL, HEAD_TOTAL, CACHED_LENGTH), jnp.float32, 0.3, 1.7)
    decay_rate = jnp.where(fast_heads, fast_rate, slow_rate) * seq_factor
    spike_mask = jax.random.uniform(every_key[5], (SEQUENCE_TOTAL, HEAD_TOTAL, CACHED_LENGTH), jnp.float32) < 3.0 / CACHED_LENGTH
    spike_length = jnp.log(jax.random.uniform(every_key[6], (SEQUENCE_TOTAL, HEAD_TOTAL, CACHED_LENGTH), jnp.float32, 0.5, 0.8))
    gate_logs = -decay_rate * coarse_scores + jnp.where(spike_mask, spike_length, 0.0)
    return jnp.cumsum(gate_logs, axis=-1).astype(jnp.float32)


def draw_expert_ids(key, part):
    group_width = EXPERTS // GROUPS
    pair_count = CAP * group_width // 2

    def one_block(block_key):
        every_key = jax.random.split(block_key, 4)
        heavy = jax.random.randint(every_key[0], (), 0, GROUPS)
        perm_keys = jax.random.split(every_key[1], GROUPS * CAP)
        orders = jax.vmap(lambda perm_key: jax.random.permutation(perm_key, group_width))(perm_keys)
        orders = orders.reshape(GROUPS, CAP * group_width).astype(jnp.int32)
        orders = orders + (jnp.arange(GROUPS, dtype=jnp.int32) * group_width)[:, None]
        pair_ids = orders.reshape(GROUPS * pair_count, 2)
        ranking = jax.random.permutation(every_key[2], GROUPS * pair_count).astype(jnp.int32)
        group_of = jnp.arange(GROUPS * pair_count, dtype=jnp.int32) // pair_count
        priority = jnp.where(group_of == heavy, 0, GROUPS * pair_count) + ranking
        chosen = jnp.argsort(priority, stable=True)[:SEQ_DEV]
        picked = pair_ids[chosen]
        shuffle = jax.random.permutation(every_key[3], SEQ_DEV)
        return picked[shuffle]
    block_keys = jax.random.split(key, SEQUENCE_TOTAL // SEQ_DEV)
    return jax.vmap(one_block)(block_keys).reshape(SEQUENCE_TOTAL, 2).astype(jnp.int32)


def with_ends(values, key, smallest, high):
    spot = [jax.random.randint(jax.random.fold_in(key, axis), (), 0, length) for axis, length in enumerate(values.shape)]
    main_axis = values.shape.index(max(values.shape))
    beside = spot[:main_axis] + [(spot[main_axis] + 1) % values.shape[main_axis]] + spot[main_axis + 1:]
    return values.at[tuple(spot)].set(smallest).at[tuple(beside)].set(high)


def shard_levels(key, shape, shards, low, high):
    factor_of = 1.0
    for axis_at, parts in shards:
        draws = jax.random.uniform(jax.random.fold_in(jax.random.fold_in(key, 6), axis_at), (parts,), jnp.float32, low / len(shards), high / len(shards))
        factor_of = factor_of * jnp.repeat(jnp.exp(draws), shape[axis_at] // parts).reshape((-1,) + (1,) * (len(shape) - 1 - axis_at))
    return factor_of


def gaussian(key, dims, scale, bound, shards=(), held_as=jnp.bfloat16):
    array = scale * jax.random.normal(key, dims, jnp.float32)
    if shards:
        array = array * shard_levels(key, dims, shards, -0.22, 0.18)
    return jnp.clip(array, -bound, bound).astype(held_as)


def setup_inputs(seed: int = 0) -> dict:
    seeds = jax.random.split(jax.random.key(seed), 24)
    return {
        "tokens": gaussian(seeds[0], (SEQUENCE_TOTAL, D), 1.0, 6.0, ((0, 32),)),
        "attn_gain": jnp.clip(1.0 + 0.18 * jax.random.normal(seeds[1], (D,), jnp.float32), 0.1, 1.9),
        "query_weight": gaussian(seeds[2], (D, HEAD_TOTAL * HEAD), D ** -0.5, 0.125, ((0, 32), (1, 16))),
        "key_weight": gaussian(seeds[3], (D, HEAD_TOTAL * HEAD), D ** -0.5, 0.125, ((0, 32), (1, 16))),
        "value_weight": gaussian(seeds[4], (D, HEAD_TOTAL * HEAD), D ** -0.5, 0.125, ((0, 32), (1, 16))),
        "forget_weight": gaussian(seeds[5], (D, HEAD_TOTAL), D ** -0.5, 0.125, ((1, 16),)),
        "forget_bias": jnp.clip(-1.0 + 3.0 * jax.random.uniform(seeds[6], (HEAD_TOTAL,), jnp.float32) ** shard_levels(seeds[6], (HEAD_TOTAL,), ((0, 16),), -0.2, 0.2), -1.0, 2.0),
        "cache_keys": draw_cache_keys(jax.random.fold_in(seeds[23], 71), 0),
        "cache_values": gaussian(seeds[8], (SEQUENCE_TOTAL, HEAD_TOTAL, CACHED_LENGTH, HEAD), 1.0, 6.0, ((0, 32), (1, 16))),
        "cache_gates": draw_cache_gates(jax.random.fold_in(seeds[23], 71), 0),
        "lengths": with_ends(jax.random.randint(seeds[10], (SEQUENCE_TOTAL,), 1, CACHED_LENGTH + 1), jax.random.fold_in(seeds[10], 1), 1, CACHED_LENGTH).astype(jnp.int32),
        "output_weight": gaussian(seeds[11], (HEAD_TOTAL * HEAD, D), (HEAD_TOTAL * HEAD) ** -0.5, 0.125, ((0, 16), (1, 32))),
        "ffn_gain": jnp.clip(1.0 + 0.18 * jax.random.normal(seeds[12], (D,), jnp.float32), 0.1, 1.9),
        "dense_gate_proj": gaussian(seeds[13], (D, FF_D), D ** -0.5, 0.125, ((0, 32), (1, 16))),
        "dense_up_proj": gaussian(seeds[14], (D, FF_D), D ** -0.5, 0.125, ((0, 32), (1, 16))),
        "dense_down_proj": gaussian(seeds[15], (FF_D, D), FF_D ** -0.5, 0.125, ((0, 16), (1, 32))),
        "dense_mix": gaussian(seeds[16], (D,), D ** -0.5, 0.125),
        "expert_ids": draw_expert_ids(jax.random.fold_in(seeds[23], 71), 0),
        "group_prob": jnp.clip(jnp.exp(math.log(1.0) - 1.3862944 * jax.random.uniform(seeds[18], (SEQUENCE_TOTAL,), jnp.float32) ** shard_levels(seeds[18], (SEQUENCE_TOTAL,), ((0, 32),), -0.2, 0.2)), 0.25, 1.0),
        "pair_prob": jnp.clip(0.05 + 0.95 * jax.random.uniform(seeds[19], (SEQUENCE_TOTAL, 2), jnp.float32) ** shard_levels(seeds[19], (SEQUENCE_TOTAL, 2), ((0, 32),), -0.2, 0.2), 0.05, 1.0),
        "expert_gate": gaussian(seeds[20], (EXPERTS, D, FF_E), D ** -0.5, 0.125, ((0, 32), (2, 16))),
        "expert_up": gaussian(seeds[21], (EXPERTS, D, FF_E), D ** -0.5, 0.125, ((0, 32), (2, 16))),
        "expert_down": gaussian(seeds[22], (EXPERTS, FF_E, D), FF_E ** -0.5, 0.125, ((0, 32), (1, 16))),
    }


EPSILON = 1e-06

def rms_scale(values, norm_gain):
    widened = values.astype(jnp.float32)
    return widened * lax.rsqrt(lax.optimization_barrier(jnp.mean(widened * widened, axis=-1, keepdims=True)) + EPSILON) * norm_gain

def attend(members):
    queries, keys_new, values_new, key_cache, value_cache, gate_cache, lengths, log_forget = members
    cache_span = key_cache.shape[2]
    score_scale = 1.0 / math.sqrt(key_cache.shape[3])
    positions = jnp.arange(cache_span, dtype=jnp.int32)
    live_mask = positions[None, :] < lengths[:, None]
    last_mask = positions[None, :] == lengths[:, None] - 1
    last_gate = lax.optimization_barrier(jnp.sum(jnp.where(last_mask[:, None, :], gate_cache, 0.0), axis=-1))
    gate_now = last_gate + log_forget
    scores = jnp.einsum('shd,shpd->shp', queries.astype(jnp.float32), key_cache.astype(jnp.float32)) * score_scale
    scores = scores + gate_now[:, :, None] - gate_cache
    scores = jnp.where(live_mask[:, None, :], scores, -jnp.inf)
    own_score = lax.optimization_barrier(jnp.sum(queries.astype(jnp.float32) * keys_new.astype(jnp.float32), axis=-1)) * score_scale
    row_top = jnp.maximum(lax.optimization_barrier(jnp.max(scores, axis=-1)), own_score)
    raised = jnp.exp(scores - row_top[:, :, None])
    own_raised = jnp.exp(own_score - row_top)
    totals = lax.optimization_barrier(jnp.sum(raised, axis=-1)) + own_raised
    weights_low = (raised / totals[:, :, None]).astype(jnp.bfloat16)
    own_prob = (own_raised / totals).astype(jnp.bfloat16)
    attended = jnp.einsum('shp,shpd->shd', weights_low.astype(jnp.float32), value_cache.astype(jnp.float32))
    attended = attended + own_prob.astype(jnp.float32)[:, :, None] * values_new.astype(jnp.float32)
    return attended.astype(jnp.bfloat16)

def by_block(array_in):
    return array_in.reshape((N_EP, array_in.shape[0] // N_EP) + array_in.shape[1:])

def reference(tokens, attn_gain, query_weight, key_weight, value_weight, forget_weight, forget_bias, cache_keys, cache_values, cache_gates, lengths, output_weight, ffn_gain, dense_gate_proj, dense_up_proj, dense_down_proj, dense_mix, expert_ids, group_prob, pair_prob, expert_gate, expert_up, expert_down):
    seq_count = tokens.shape[0]
    normed = rms_scale(tokens, attn_gain).astype(jnp.bfloat16)
    queries = jnp.dot(normed, query_weight, preferred_element_type=jnp.float32).astype(jnp.bfloat16)
    keys_new = jnp.dot(normed, key_weight, preferred_element_type=jnp.float32).astype(jnp.bfloat16)
    values_new = jnp.dot(normed, value_weight, preferred_element_type=jnp.float32).astype(jnp.bfloat16)
    queries = queries.reshape(seq_count, HEAD_TOTAL, HEAD)
    keys_new = keys_new.reshape(seq_count, HEAD_TOTAL, HEAD)
    values_new = values_new.reshape(seq_count, HEAD_TOTAL, HEAD)
    log_forget = jax.nn.log_sigmoid(jnp.dot(normed, forget_weight, preferred_element_type=jnp.float32) + forget_bias)
    members = tuple((by_block(item) for item in (queries, keys_new, values_new, cache_keys, cache_values, cache_gates, lengths, log_forget)))
    attended = lax.map(attend, members).reshape(seq_count, HEAD_TOTAL * HEAD)
    residual = (tokens.astype(jnp.float32) + jnp.dot(attended, output_weight, preferred_element_type=jnp.float32)).astype(jnp.bfloat16)
    ffn_in = rms_scale(residual, ffn_gain).astype(jnp.bfloat16)
    dense_gate_part = jnp.dot(ffn_in, dense_gate_proj, preferred_element_type=jnp.float32)
    dense_up_part = jnp.dot(ffn_in, dense_up_proj, preferred_element_type=jnp.float32)
    dense_hidden = (jax.nn.silu(dense_gate_part) * dense_up_part).astype(jnp.bfloat16)
    dense_total = jnp.dot(dense_hidden, dense_down_proj, preferred_element_type=jnp.float32)
    mix = jax.nn.sigmoid(jnp.dot(ffn_in, dense_mix, preferred_element_type=jnp.float32))
    routes = group_prob[:, None] * pair_prob / lax.optimization_barrier(jnp.sum(pair_prob, axis=1, keepdims=True))
    most_rows = CAP * N_EP

    def one_expert(accum, expert_index):
        hit_mask = expert_ids == expert_index
        row_weight = lax.optimization_barrier(jnp.sum(jnp.where(hit_mask, routes, 0.0), axis=1))
        any_hit = lax.optimization_barrier(jnp.sum(hit_mask.astype(jnp.int32), axis=1)) > 0
        chosen = jnp.nonzero(any_hit, size=most_rows, fill_value=0)[0].astype(jnp.int32)
        valid_rows = jnp.arange(most_rows, dtype=jnp.int32) < jnp.sum(any_hit.astype(jnp.int32))
        row_data = ffn_in[chosen]
        gate_part = jnp.dot(row_data, expert_gate[expert_index], preferred_element_type=jnp.float32)
        up_part = jnp.dot(row_data, expert_up[expert_index], preferred_element_type=jnp.float32)
        expert_hidden = (jax.nn.silu(gate_part) * up_part).astype(jnp.bfloat16)
        expert_out = jnp.dot(expert_hidden, expert_down[expert_index], preferred_element_type=jnp.float32)
        weight_rows = jnp.where(valid_rows, row_weight[chosen], 0.0)
        return (accum.at[chosen].add(weight_rows[:, None] * expert_out), None)
    expert_sum, _ = lax.scan(one_expert, jnp.zeros((seq_count, D), jnp.float32), jnp.arange(EXPERTS, dtype=jnp.int32))
    result = residual.astype(jnp.float32) + expert_sum + mix[:, None] * dense_total
    return result.astype(jnp.bfloat16)
```

```python
import math

import jax
import jax.numpy as jnp
from jax import lax
from jax.sharding import Mesh
from jax.sharding import PartitionSpec as P

EP = ("zh", "zl", "c")
Z = ("zh", "zl")
TP = ("y", "x")
EPSILON = 1e-06


def exchanged(pieces, axes):
    return lax.all_to_all(pieces, axes, split_axis=0, concat_axis=0, tiled=True)


def summed_over(array, axes):
    copies = jnp.broadcast_to(array, (lax.axis_size(axes), *array.shape))
    return jnp.sum(exchanged(copies, axes).astype(jnp.float32), axis=0)


def product(left, right):
    return jnp.dot(left, right, preferred_element_type=jnp.float32)


def product_transposed(left, right):
    return lax.dot_general(
        left, right, (((1,), (1,)), ((), ())), preferred_element_type=jnp.float32
    )


def rms_scale(values, norm_gain):
    widened = values.astype(jnp.float32)
    return (
        widened
        * lax.rsqrt(jnp.mean(widened * widened, axis=-1, keepdims=True) + EPSILON)
        * norm_gain
    )


def attend(queries, keys_new, values_new, key_cache, value_cache, gate_cache, lengths, log_forget):
    cache_span = key_cache.shape[2]
    score_scale = 1.0 / math.sqrt(key_cache.shape[3])
    positions = jnp.arange(cache_span, dtype=jnp.int32)
    live_mask = positions[None, :] < lengths[:, None]
    last_mask = positions[None, :] == lengths[:, None] - 1
    last_gate = jnp.sum(jnp.where(last_mask[:, None, :], gate_cache, 0.0), axis=-1)
    gate_now = last_gate + log_forget
    scores = (
        jnp.einsum("shd,shpd->shp", queries, key_cache, preferred_element_type=jnp.float32)
        * score_scale
    )
    scores = scores + gate_now[:, :, None] - gate_cache
    scores = jnp.where(live_mask[:, None, :], scores, -jnp.inf)
    own_score = (
        jnp.sum(queries.astype(jnp.float32) * keys_new.astype(jnp.float32), axis=-1) * score_scale
    )
    row_top = jnp.maximum(jnp.max(scores, axis=-1), own_score)
    raised = jnp.exp(scores - row_top[:, :, None])
    own_raised = jnp.exp(own_score - row_top)
    totals = jnp.sum(raised, axis=-1) + own_raised
    weights_low = (raised / totals[:, :, None]).astype(jnp.bfloat16)
    own_prob = (own_raised / totals).astype(jnp.bfloat16)
    attended = jnp.einsum(
        "shp,shpd->shd", weights_low, value_cache, preferred_element_type=jnp.float32
    )
    attended = attended + own_prob.astype(jnp.float32)[:, :, None] * values_new.astype(jnp.float32)
    return attended.astype(jnp.bfloat16)


def shards(
    tokens,
    attn_gain,
    query_weight,
    key_weight,
    value_weight,
    forget_weight,
    forget_bias,
    cache_keys,
    cache_values,
    cache_gates,
    lengths,
    output_weight,
    ffn_gain,
    dense_gate_proj,
    dense_up_proj,
    dense_down_proj,
    dense_mix,
    expert_ids,
    group_prob,
    pair_prob,
    expert_gate,
    expert_up,
    expert_down,
):
    seq_count, width = tokens.shape
    head_size = cache_keys.shape[3]
    chips = lax.axis_size(Z)
    quarters = lax.axis_size("zl")
    devices = lax.axis_size(EP)
    slab = width // chips
    core = lax.axis_index("c")

    own_rows = jnp.concatenate(
        (query_weight, key_weight, value_weight, dense_gate_proj, dense_up_proj), axis=1
    )
    their_rows = lax.ppermute(own_rows, "c", [(0, 1), (1, 0)])
    chip_rows = jnp.where(
        core == 0,
        jnp.concatenate((own_rows, their_rows), axis=0),
        jnp.concatenate((their_rows, own_rows), axis=0),
    )
    projection_width = 3 * head_size

    normed = rms_scale(tokens, attn_gain).astype(jnp.bfloat16)
    token_pieces = normed.reshape(seq_count, chips, slab).transpose(1, 0, 2)
    held = output_weight.shape[1]
    part = held // quarters
    out_parts = output_weight.T.reshape(quarters, part, head_size)
    down_parts = dense_down_proj.T.reshape(quarters, part, head_size)
    parts = jnp.tile(jnp.concatenate((out_parts, down_parts), axis=1), (chips // quarters, 1, 1))
    received = exchanged(jnp.concatenate((token_pieces, parts), axis=1), Z)
    token_columns = received[:, :seq_count].reshape(chips * seq_count, slab)
    out_quarter = received[:, seq_count : seq_count + part]
    down_quarter = received[:, seq_count + part :]

    def whole(quarter):
        gathered = lax.all_gather(quarter, ("zl", "c"), axis=0, tiled=False)
        gathered = gathered.reshape(quarters, 2, chips, part, head_size)
        return gathered.transpose(2, 1, 0, 3, 4).reshape(width, head_size)

    shares = product(token_columns, chip_rows[:, :projection_width]).astype(jnp.bfloat16)
    shares = exchanged(shares.reshape(chips, seq_count, projection_width), Z)
    output_columns = whole(out_quarter)
    projected = jnp.sum(shares.astype(jnp.float32), axis=0).astype(jnp.bfloat16)
    projected = projected.reshape(seq_count, 3, 1, head_size)
    log_forget = jax.nn.log_sigmoid(product(normed, forget_weight) + forget_bias)
    attended = attend(
        projected[:, 0],
        projected[:, 1],
        projected[:, 2],
        cache_keys,
        cache_values,
        cache_gates,
        lengths,
        log_forget,
    ).reshape(seq_count, head_size)
    head_terms = product_transposed(attended, output_columns).astype(jnp.bfloat16)
    down_columns = whole(down_quarter)
    residual = (tokens.astype(jnp.float32) + summed_over(head_terms, TP)).astype(jnp.bfloat16)
    ffn_in = rms_scale(residual, ffn_gain).astype(jnp.bfloat16)
    mix = jax.nn.sigmoid(product(ffn_in, dense_mix))

    picks = expert_ids.reshape(-1)
    capacity = 4 * seq_count // devices
    slot_total = devices * capacity
    pick_onehot = (picks[:, None] == jnp.arange(devices, dtype=jnp.int32)[None, :]).astype(jnp.int32)
    earlier = jnp.cumsum(pick_onehot, axis=0) - pick_onehot
    slot_rank = jnp.sum(earlier * pick_onehot, axis=1)
    destination = (picks * capacity + slot_rank).reshape(seq_count, 2)
    slot_grid = jnp.arange(slot_total, dtype=jnp.int32)
    select_first = (destination[:, 0:1] == slot_grid[None, :]).astype(jnp.bfloat16)
    select_second = (destination[:, 1:2] == slot_grid[None, :]).astype(jnp.bfloat16)
    outbound = jnp.einsum(
        "sk,sd->kd", select_first + select_second, ffn_in, preferred_element_type=jnp.float32
    )
    outbound = outbound.astype(jnp.bfloat16).reshape(devices, capacity, width)
    half = seq_count // 2
    across = half // capacity
    dense_pieces = ffn_in.reshape(2, across, capacity, chips, slab).transpose(3, 0, 2, 1, 4)
    dense_pieces = dense_pieces.reshape(devices, capacity, across * slab)
    arrived = exchanged(jnp.concatenate((outbound, dense_pieces), axis=2), EP)
    row_data = arrived[:, :, :width].reshape(slot_total, width)
    dense_rows = arrived[:, :, width:].reshape(devices, capacity, across, slab)
    dense_rows = dense_rows.transpose(0, 2, 1, 3).reshape(devices * half, slab)

    dense_shares = product(dense_rows, chip_rows[:, projection_width:]).astype(jnp.bfloat16)
    dense_width = dense_shares.shape[1]
    dense_shares = dense_shares.reshape(devices, capacity, across * dense_width)
    gate_part = product(row_data, expert_gate[0])
    up_part = product(row_data, expert_up[0])
    expert_hidden = (jax.nn.silu(gate_part) * up_part).astype(jnp.bfloat16)
    partial_out = product(expert_hidden, expert_down[0]).astype(jnp.bfloat16)
    back = exchanged(
        jnp.concatenate((partial_out.reshape(devices, capacity, width), dense_shares), axis=2), EP
    )
    returned = back[:, :, :width].reshape(slot_total, width)
    dense_parts = back[:, :, width:].reshape(chips, seq_count, dense_width)
    dense_parts = jnp.sum(dense_parts.astype(jnp.float32), axis=0)
    dense_hidden = jax.nn.silu(dense_parts[:, :head_size]) * dense_parts[:, head_size:]
    dense_terms = product_transposed(dense_hidden.astype(jnp.bfloat16), down_columns)
    routes = group_prob[:, None] * pair_prob / jnp.sum(pair_prob, axis=1, keepdims=True)
    side_total = (
        routes[:, 0:1] * product(select_first, returned)
        + routes[:, 1:2] * product(select_second, returned)
        + mix[:, None] * dense_terms
    )
    result = residual.astype(jnp.float32) + summed_over(side_total.astype(jnp.bfloat16), TP)
    return result.astype(jnp.bfloat16)


def solution(mesh):
    chips = mesh.shape["ep"] // 2
    finer = Mesh(mesh.devices.reshape(chips // 4, 4, 2, 4, 4), ("zh", "zl", "c", "y", "x"))
    in_specs = (
        P(EP, None),
        P(),
        P(EP, TP),
        P(EP, TP),
        P(EP, TP),
        P(None, TP),
        P(TP),
        P(EP, TP, None, None),
        P(EP, TP, None, None),
        P(EP, TP, None),
        P(EP),
        P(TP, EP),
        P(),
        P(EP, TP),
        P(EP, TP),
        P(TP, EP),
        P(),
        P(EP, None),
        P(EP),
        P(EP, None),
        P(EP, None, TP),
        P(EP, None, TP),
        P(EP, TP, None),
    )
    out_specs = P(EP, None)
    return jax.shard_map(
        shards, mesh=finer, in_specs=in_specs, out_specs=out_specs, check_vma=False
    )
```

```python
import math

import jax
import jax.numpy as jnp
from jax import lax
from jax.sharding import Mesh
from jax.sharding import PartitionSpec as P


EP = ("zh", "zl", "c")
Z = ("zh", "zl")
TP = ("y", "x")
EPSILON = 1e-06


def exchanged(pieces, axes):
    return lax.all_to_all(pieces, axes, split_axis=0, concat_axis=0, tiled=True)


def from_all(array, axis):
    return exchanged(jnp.broadcast_to(array, (lax.axis_size(axis), *array.shape)), axis)


def summed_over_heads(array):
    rows = jnp.sum(from_all(array, "x").astype(jnp.float32), axis=0).astype(jnp.bfloat16)
    return jnp.sum(from_all(rows, "y").astype(jnp.float32), axis=0)


def in_order(own, theirs, place, dim):
    return jnp.where(
        place == 0,
        jnp.concatenate((own, theirs), axis=dim),
        jnp.concatenate((theirs, own), axis=dim),
    )


def product(left, right):
    return jnp.dot(left, right, preferred_element_type=jnp.float32)


def product_transposed(left, right):
    return lax.dot_general(
        left, right, (((1,), (1,)), ((), ())), preferred_element_type=jnp.float32
    )


def rms_scale(values, norm_gain):
    widened = values.astype(jnp.float32)
    return (
        widened
        * lax.rsqrt(jnp.mean(widened * widened, axis=-1, keepdims=True) + EPSILON)
        * norm_gain
    )


def attend(queries, keys_new, values_new, key_cache, value_cache, gate_cache, lengths, log_forget):
    cache_span = key_cache.shape[2]
    score_scale = 1.0 / math.sqrt(key_cache.shape[3])
    positions = jnp.arange(cache_span, dtype=jnp.int32)
    live_mask = positions[None, :] < lengths[:, None]
    last_mask = positions[None, :] == lengths[:, None] - 1
    last_gate = jnp.sum(jnp.where(last_mask[:, None, :], gate_cache, 0.0), axis=-1)
    gate_now = last_gate + log_forget
    scores = (
        jnp.einsum("shd,shpd->shp", queries, key_cache, preferred_element_type=jnp.float32)
        * score_scale
    )
    scores = scores + gate_now[:, :, None] - gate_cache
    scores = jnp.where(live_mask[:, None, :], scores, -jnp.inf)
    own_score = (
        jnp.sum(queries.astype(jnp.float32) * keys_new.astype(jnp.float32), axis=-1) * score_scale
    )
    row_top = jnp.maximum(jnp.max(scores, axis=-1), own_score)
    raised = jnp.exp(scores - row_top[:, :, None])
    own_raised = jnp.exp(own_score - row_top)
    totals = jnp.sum(raised, axis=-1) + own_raised
    weights_low = (raised / totals[:, :, None]).astype(jnp.bfloat16)
    own_prob = (own_raised / totals).astype(jnp.bfloat16)
    attended = jnp.einsum(
        "shp,shpd->shd", weights_low, value_cache, preferred_element_type=jnp.float32
    )
    attended = attended + own_prob.astype(jnp.float32)[:, :, None] * values_new.astype(jnp.float32)
    return attended.astype(jnp.bfloat16)


def layer(
    tokens,
    attn_gain,
    query_weight,
    key_weight,
    value_weight,
    forget_weight,
    forget_bias,
    cache_keys,
    cache_values,
    cache_gates,
    lengths,
    output_weight,
    ffn_gain,
    dense_gate_proj,
    dense_up_proj,
    dense_down_proj,
    dense_mix,
    expert_ids,
    group_prob,
    pair_prob,
    expert_gate,
    expert_up,
    expert_down,
):
    seq_count, width = tokens.shape
    head_size = cache_keys.shape[3]
    chips = lax.axis_size(Z)
    quarters = lax.axis_size("zl")
    devices = lax.axis_size(EP)
    slab = width // chips
    core = lax.axis_index("c")
    side = lax.axis_index("zl") % 2
    pairs = chips // 2
    half = seq_count // 2

    own_rows = jnp.concatenate(
        (query_weight, key_weight, value_weight, dense_gate_proj, dense_up_proj), axis=1
    )
    chip_rows = in_order(own_rows, lax.ppermute(own_rows, "c", [(0, 1), (1, 0)]), core, 0)
    neighbours = [(k, k ^ 1) for k in range(quarters)]
    pair_rows = in_order(chip_rows, lax.ppermute(chip_rows, "zl", neighbours), side, 0)
    projection_width = 3 * head_size

    normed = rms_scale(tokens, attn_gain).astype(jnp.bfloat16)
    token_pieces = normed.reshape(2, half, pairs, 2, slab).transpose(2, 0, 3, 1, 4)
    token_pieces = token_pieces.reshape(chips, seq_count, slab)
    held = output_weight.shape[1]
    part = held // quarters
    out_parts = output_weight.T.reshape(quarters, part, head_size)
    down_parts = dense_down_proj.T.reshape(quarters, part, head_size)
    parts = jnp.tile(jnp.concatenate((out_parts, down_parts), axis=1), (chips // quarters, 1, 1))
    received = exchanged(jnp.concatenate((token_pieces, parts), axis=1), Z)
    token_columns = received[:, :seq_count].reshape(chips, 2, half, slab)
    token_columns = token_columns.transpose(0, 2, 1, 3).reshape(chips * half, 2 * slab)
    quarter = received[:, seq_count:]
    both = in_order(
        quarter[:, None], lax.ppermute(quarter, "c", [(0, 1), (1, 0)])[:, None], core, 1
    )

    def whole(pieces):
        gathered = lax.all_gather(pieces, "zl", axis=0, tiled=False)
        return gathered.transpose(1, 2, 0, 3, 4).reshape(width, head_size)

    shares = product(token_columns, pair_rows[:, :projection_width]).astype(jnp.bfloat16)
    shares = exchanged(shares.reshape(chips, half, projection_width), Z)
    output_columns = whole(both[:, :, :part])
    shares = shares.reshape(pairs, seq_count, projection_width)
    projected = jnp.sum(shares.astype(jnp.float32), axis=0).astype(jnp.bfloat16)
    projected = projected.reshape(seq_count, 3, 1, head_size)
    log_forget = jax.nn.log_sigmoid(product(normed, forget_weight) + forget_bias)
    attended = attend(
        projected[:, 0],
        projected[:, 1],
        projected[:, 2],
        cache_keys,
        cache_values,
        cache_gates,
        lengths,
        log_forget,
    ).reshape(seq_count, head_size)
    picks = expert_ids.reshape(-1)
    capacity = 4 * seq_count // devices
    slot_total = devices * capacity
    pick_onehot = (picks[:, None] == jnp.arange(devices, dtype=jnp.int32)[None, :]).astype(jnp.int32)
    earlier = jnp.cumsum(pick_onehot, axis=0) - pick_onehot
    slot_rank = jnp.sum(earlier * pick_onehot, axis=1)
    destination = (picks * capacity + slot_rank).reshape(seq_count, 2)
    slot_grid = jnp.arange(slot_total, dtype=jnp.int32)
    select_first = (destination[:, 0:1] == slot_grid[None, :]).astype(jnp.bfloat16)
    select_second = (destination[:, 1:2] == slot_grid[None, :]).astype(jnp.bfloat16)
    routes = group_prob[:, None] * pair_prob / jnp.sum(pair_prob, axis=1, keepdims=True)
    head_terms = product_transposed(attended, output_columns).astype(jnp.bfloat16)
    lane = lax.axis_index("x")
    share = width // lax.axis_size("x")
    head_terms, selectors, routes, lane, share_start = lax.optimization_barrier(
        (head_terms, (select_first, select_second), routes, lane, lane * share)
    )
    select_first, select_second = selectors
    residual = (tokens.astype(jnp.float32) + summed_over_heads(head_terms)).astype(jnp.bfloat16)
    ffn_in = rms_scale(residual, ffn_gain).astype(jnp.bfloat16)
    mix = jax.nn.sigmoid(product(ffn_in, dense_mix))

    lanes = lax.axis_size("x")
    ffn_share = lax.dynamic_slice_in_dim(
        ffn_in, share_start, share, axis=1, allow_negative_indices=False
    )
    outbound = jnp.einsum(
        "sk,sd->kd", select_first + select_second, ffn_share, preferred_element_type=jnp.float32
    )
    outbound = outbound.astype(jnp.bfloat16).reshape(devices, capacity, share)
    few = seq_count // 4
    dense_pieces = ffn_in.reshape(4, few, pairs, 2, slab)
    dense_pieces = lax.dynamic_index_in_dim(
        dense_pieces, lane, axis=1, keepdims=False, allow_negative_indices=False
    )
    dense_pieces = dense_pieces.transpose(1, 0, 2, 3).reshape(devices, 2, slab)
    arrived = exchanged(jnp.concatenate((outbound, dense_pieces), axis=2), EP)
    arrived = from_all(arrived, "x")
    row_data = jnp.concatenate(
        [arrived[k, :, :, :share].reshape(slot_total, share) for k in range(lanes)], axis=1
    )
    dense_rows = arrived[:, :, :, share:].transpose(1, 0, 2, 3).reshape(devices * few, 2 * slab)

    dense_shares = product(dense_rows, pair_rows[:, projection_width:]).astype(jnp.bfloat16)
    dense_width = dense_shares.shape[1]
    dense_shares = dense_shares.reshape(devices, capacity, few // capacity * dense_width)
    gate_part = product(row_data, expert_gate[0])
    up_part = product(row_data, expert_up[0])
    expert_hidden = (jax.nn.silu(gate_part) * up_part).astype(jnp.bfloat16)
    partial_out = product(expert_hidden, expert_down[0]).astype(jnp.bfloat16)
    back = exchanged(
        jnp.concatenate((partial_out.reshape(devices, capacity, width), dense_shares), axis=2),
        EP,
    )
    down_columns = whole(both[:, :, part:])
    returned = back[:, :, :width].reshape(slot_total, width)
    dense_parts = back[:, :, width:].reshape(pairs, seq_count, dense_width)
    dense_parts = jnp.sum(dense_parts.astype(jnp.float32), axis=0)
    dense_hidden = jax.nn.silu(dense_parts[:, :head_size]) * dense_parts[:, head_size:]
    dense_terms = product_transposed(dense_hidden.astype(jnp.bfloat16), down_columns)
    side_total = (
        routes[:, 0:1] * product(select_first, returned)
        + routes[:, 1:2] * product(select_second, returned)
        + mix[:, None] * dense_terms
    )
    result = residual.astype(jnp.float32) + summed_over_heads(side_total.astype(jnp.bfloat16))
    return result.astype(jnp.bfloat16)


def solution(mesh):
    chips = mesh.shape["ep"] // 2
    finer = Mesh(mesh.devices.reshape(chips // 4, 4, 2, 4, 4), ("zh", "zl", "c", "y", "x"))
    in_specs = (
        P(EP, None),
        P(),
        P(EP, TP),
        P(EP, TP),
        P(EP, TP),
        P(None, TP),
        P(TP),
        P(EP, TP, None, None),
        P(EP, TP, None, None),
        P(EP, TP, None),
        P(EP),
        P(TP, EP),
        P(),
        P(EP, TP),
        P(EP, TP),
        P(TP, EP),
        P(),
        P(EP, None),
        P(EP),
        P(EP, None),
        P(EP, None, TP),
        P(EP, None, TP),
        P(EP, TP, None),
    )
    out_specs = P(EP, None)
    return jax.shard_map(layer, mesh=finer, in_specs=in_specs, out_specs=out_specs, check_vma=False)
```

```python
import math

import jax
import jax.numpy as jnp
from jax import lax
from jax.experimental import pallas as pl
from jax.experimental.pallas import tpu as pltpu
from jax.sharding import Mesh
from jax.sharding import PartitionSpec as P


EP = ("zh", "zl", "c")
Z = ("zh", "zl")
TP = ("y", "x")
EPSILON = 1e-06


def exchanged(pieces, axes):
    return lax.all_to_all(pieces, axes, split_axis=0, concat_axis=0, tiled=True)


def from_all(array, axis):
    return exchanged(jnp.broadcast_to(array, (lax.axis_size(axis), *array.shape)), axis)


def summed_over_heads(array):
    rows = jnp.sum(from_all(array, "x").astype(jnp.float32), axis=0).astype(jnp.bfloat16)
    return jnp.sum(from_all(rows, "y").astype(jnp.float32), axis=0)


def in_order(own, theirs, place, dim):
    return jnp.where(
        place == 0,
        jnp.concatenate((own, theirs), axis=dim),
        jnp.concatenate((theirs, own), axis=dim),
    )


def product(left, right):
    return jnp.dot(left, right, preferred_element_type=jnp.float32)


def product_transposed(left, right):
    return lax.dot_general(
        left, right, (((1,), (1,)), ((), ())), preferred_element_type=jnp.float32
    )


def rms_scale(values, norm_gain):
    widened = values.astype(jnp.float32)
    return (
        widened
        * lax.rsqrt(jnp.mean(widened * widened, axis=-1, keepdims=True) + EPSILON)
        * norm_gain
    )


def first_payload(tokens_ref, gain_ref, out_ref, down_ref, payload_ref, normed_ref):
    seq_count, _ = tokens_ref.shape
    chips, _, slab = payload_ref.shape
    half = seq_count // 2
    held = out_ref.shape[0]
    widened = tokens_ref[...].astype(jnp.float32)
    mean = jnp.mean(widened * widened, axis=-1, keepdims=True)
    normed = (widened * lax.rsqrt(mean + EPSILON) * gain_ref[...]).astype(jnp.bfloat16)
    normed_ref[...] = normed
    for chip in range(chips):
        pair, side = divmod(chip, 2)
        for k in range(2):
            first = (2 * pair + k) * slab
            payload_ref[chip, k * half : (k + 1) * half, :] = normed[
                side * half : (side + 1) * half, first : first + slab
            ]
        row = seq_count
        payload_ref[chip, row : row + held // 2, :] = out_ref[
            side * (held // 2) : (side + 1) * (held // 2), :
        ]
        row += held // 2
        quarter = chip % 4
        payload_ref[chip, row : row + held // 4, :] = down_ref[
            quarter * (held // 4) : (quarter + 1) * (held // 4), :
        ]


def experts(
    rows_ref, dense_ref, gate_hbm, up_hbm, down_hbm, payload_ref,
    gate_ref, up_ref, down_ref, low_ref, high_ref, mixed_ref, sems,
):
    lanes, slots, _ = rows_ref.shape
    width, hidden_width = gate_ref.shape
    share = width // lanes
    slab = dense_ref.shape[0] // 2
    dense_width = hidden_width * 2
    first = dense_ref.shape[1] - dense_width
    copies = [
        pltpu.make_async_copy(source, target, sems.at[k])
        for k, (source, target) in enumerate(
            ((gate_hbm, gate_ref), (up_hbm, up_ref), (down_hbm, down_ref))
        )
    ]
    for copy in copies:
        copy.start()
    for lane in range(lanes):
        pieces = rows_ref[lane, :, share : share + slab]
        low = jnp.dot(pieces, dense_ref[:slab, first:], preferred_element_type=jnp.float32)
        high = jnp.dot(pieces, dense_ref[slab:, first:], preferred_element_type=jnp.float32)
        row, place = divmod(lane, 2)
        for part in range(2):
            span = slice(part * hidden_width, (part + 1) * hidden_width)
            low_ref[part] = low[:, span]
            high_ref[part] = high[:, span]
            mixed_ref[2 * place + part, pl.ds(row, slots // 2, stride=2), :] = (
                low_ref[part, pl.ds(0, slots // 2, stride=2), :]
                + high_ref[part, pl.ds(1, slots // 2, stride=2), :]
            )
    for part in range(mixed_ref.shape[0]):
        span = slice(width + part * hidden_width, width + (part + 1) * hidden_width)
        payload_ref[:, span] = mixed_ref[part].astype(jnp.bfloat16)
    copies[0].wait()
    copies[1].wait()
    gate_part = jnp.zeros((slots, hidden_width), jnp.float32)
    up_part = jnp.zeros((slots, hidden_width), jnp.float32)
    for lane in range(lanes):
        rows = rows_ref[lane, :, :share]
        span = slice(lane * share, (lane + 1) * share)
        gate_part += jnp.dot(rows, gate_ref[span, :], preferred_element_type=jnp.float32)
        up_part += jnp.dot(rows, up_ref[span, :], preferred_element_type=jnp.float32)
    hidden = (gate_part / (1.0 + jnp.exp(-gate_part)) * up_part).astype(jnp.bfloat16)
    copies[2].wait()
    payload_ref[:, :width] = jnp.dot(
        hidden, down_ref[...], preferred_element_type=jnp.float32
    ).astype(jnp.bfloat16)


def attend(queries, keys_new, values_new, key_cache, value_cache, gate_cache, lengths, log_forget):
    cache_span = key_cache.shape[2]
    score_scale = 1.0 / math.sqrt(key_cache.shape[3])
    positions = jnp.arange(cache_span, dtype=jnp.int32)
    live_mask = positions[None, :] < lengths[:, None]
    last_mask = positions[None, :] == lengths[:, None] - 1
    last_gate = jnp.sum(jnp.where(last_mask[:, None, :], gate_cache, 0.0), axis=-1)
    gate_now = last_gate + log_forget
    scores = (
        jnp.einsum("shd,shpd->shp", queries, key_cache, preferred_element_type=jnp.float32)
        * score_scale
    )
    scores = scores + gate_now[:, :, None] - gate_cache
    scores = jnp.where(live_mask[:, None, :], scores, -jnp.inf)
    own_score = (
        jnp.sum(queries.astype(jnp.float32) * keys_new.astype(jnp.float32), axis=-1) * score_scale
    )
    row_top = jnp.maximum(jnp.max(scores, axis=-1), own_score)
    raised = jnp.exp(scores - row_top[:, :, None])
    own_raised = jnp.exp(own_score - row_top)
    totals = jnp.sum(raised, axis=-1) + own_raised
    weights_low = (raised / totals[:, :, None]).astype(jnp.bfloat16)
    own_prob = (own_raised / totals).astype(jnp.bfloat16)
    attended = jnp.einsum(
        "shp,shpd->shd", weights_low, value_cache, preferred_element_type=jnp.float32
    )
    attended = attended + own_prob.astype(jnp.float32)[:, :, None] * values_new.astype(jnp.float32)
    return attended.astype(jnp.bfloat16)


def layer(
    tokens,
    attn_gain,
    query_weight,
    key_weight,
    value_weight,
    forget_weight,
    forget_bias,
    cache_keys,
    cache_values,
    cache_gates,
    lengths,
    output_weight,
    ffn_gain,
    dense_gate_proj,
    dense_up_proj,
    dense_down_proj,
    dense_mix,
    expert_ids,
    group_prob,
    pair_prob,
    expert_gate,
    expert_up,
    expert_down,
):
    seq_count, width = tokens.shape
    head_size = cache_keys.shape[3]
    chips = lax.axis_size(Z)
    quarters = lax.axis_size("zl")
    devices = lax.axis_size(EP)
    slab = width // chips
    core = lax.axis_index("c")
    side = lax.axis_index("zl") % 2
    pairs = chips // 2
    half = seq_count // 2

    own_rows = jnp.concatenate(
        (query_weight, key_weight, value_weight, dense_gate_proj, dense_up_proj), axis=1
    )
    chip_rows = in_order(own_rows, lax.ppermute(own_rows, "c", [(0, 1), (1, 0)]), core, 0)
    neighbours = [(k, k ^ 1) for k in range(quarters)]
    pair_rows = in_order(chip_rows, lax.ppermute(chip_rows, "zl", neighbours), side, 0)
    projection_width = 3 * head_size

    held = output_weight.shape[1]
    part = held // quarters
    vmem = pl.BlockSpec(memory_space=pltpu.VMEM)
    payload, normed = pl.pallas_call(
        first_payload,
        out_shape=(
            jax.ShapeDtypeStruct((chips, seq_count + held // 2 + part, slab), jnp.bfloat16),
            jax.ShapeDtypeStruct((seq_count, width), jnp.bfloat16),
        ),
        in_specs=(vmem,) * 4,
        out_specs=(vmem,) * 2,
        name="first_payload",
    )(tokens, attn_gain[None], output_weight.T, dense_down_proj.T)
    received = exchanged(payload, Z)
    token_columns = received[:, :seq_count].reshape(chips, 2, half, slab)
    token_columns = token_columns.transpose(0, 2, 1, 3).reshape(chips * half, 2 * slab)
    out_half = received[:, seq_count : seq_count + held // 2]
    down_quarter = received[:, seq_count + held // 2 :]
    swap = [(0, 1), (1, 0)]

    out_held = in_order(
        out_half[:, None], lax.ppermute(out_half, "zl", neighbours)[:, None], side, 1
    )
    out_all = in_order(out_held[:, None], lax.ppermute(out_held, "c", swap)[:, None], core, 1)
    output_columns = out_all.reshape(width, head_size)

    shares = product(token_columns, pair_rows[:, :projection_width]).astype(jnp.bfloat16)
    shares = exchanged(shares.reshape(chips, half, projection_width), Z)
    shares = shares.reshape(pairs, seq_count, projection_width)
    projected = jnp.sum(shares.astype(jnp.float32), axis=0).astype(jnp.bfloat16)
    projected = projected.reshape(seq_count, 3, 1, head_size)
    log_forget = jax.nn.log_sigmoid(product(normed, forget_weight) + forget_bias)
    attended = attend(
        projected[:, 0],
        projected[:, 1],
        projected[:, 2],
        cache_keys,
        cache_values,
        cache_gates,
        lengths,
        log_forget,
    ).reshape(seq_count, head_size)
    picks = expert_ids.reshape(-1)
    capacity = 4 * seq_count // devices
    slot_total = devices * capacity
    pick_onehot = (picks[:, None] == jnp.arange(devices, dtype=jnp.int32)[None, :]).astype(jnp.int32)
    earlier = jnp.cumsum(pick_onehot, axis=0) - pick_onehot
    slot_rank = jnp.sum(earlier * pick_onehot, axis=1)
    destination = (picks * capacity + slot_rank).reshape(seq_count, 2)
    slot_grid = jnp.arange(slot_total, dtype=jnp.int32)
    select_first = (destination[:, 0:1] == slot_grid[None, :]).astype(jnp.bfloat16)
    select_second = (destination[:, 1:2] == slot_grid[None, :]).astype(jnp.bfloat16)
    routes = group_prob[:, None] * pair_prob / jnp.sum(pair_prob, axis=1, keepdims=True)
    head_terms = product_transposed(attended, output_columns).astype(jnp.bfloat16)
    lane = lax.axis_index("x")
    share = width // lax.axis_size("x")
    head_terms, selectors, routes, lane, share_start = lax.optimization_barrier(
        (head_terms, (select_first, select_second), routes, lane, lane * share)
    )
    select_first, select_second = selectors
    residual = (tokens.astype(jnp.float32) + summed_over_heads(head_terms)).astype(jnp.bfloat16)
    ffn_in = rms_scale(residual, ffn_gain).astype(jnp.bfloat16)
    mix = jax.nn.sigmoid(product(ffn_in, dense_mix))

    lanes = lax.axis_size("x")
    ffn_share = lax.dynamic_slice_in_dim(
        ffn_in, share_start, share, axis=1, allow_negative_indices=False
    )
    outbound = jnp.einsum(
        "sk,sd->kd", select_first + select_second, ffn_share, preferred_element_type=jnp.float32
    )
    outbound = outbound.astype(jnp.bfloat16).reshape(devices, capacity, share)
    few = seq_count // 4
    dense_pieces = ffn_in.reshape(4, few, pairs, 2, slab)
    dense_pieces = lax.dynamic_index_in_dim(
        dense_pieces, lane, axis=1, keepdims=False, allow_negative_indices=False
    )
    dense_pieces = dense_pieces.transpose(1, 0, 2, 3).reshape(devices, 2, slab)
    arrived = exchanged(jnp.concatenate((outbound, dense_pieces), axis=2), EP)
    arrived = from_all(arrived, "x")
    dense_width = 2 * head_size
    payload_width = width + few // capacity * dense_width
    hbm = pl.BlockSpec(memory_space=pl.ANY)
    payload = pl.pallas_call(
        experts,
        out_shape=jax.ShapeDtypeStruct((slot_total, payload_width), jnp.bfloat16),
        in_specs=(vmem, vmem, hbm, hbm, hbm),
        out_specs=vmem,
        scratch_shapes=(
            pltpu.VMEM(expert_gate.shape[1:], jnp.bfloat16),
            pltpu.VMEM(expert_up.shape[1:], jnp.bfloat16),
            pltpu.VMEM(expert_down.shape[1:], jnp.bfloat16),
            pltpu.VMEM((2, slot_total, head_size), jnp.float32),
            pltpu.VMEM((2, slot_total, head_size), jnp.float32),
            pltpu.VMEM(((payload_width - width) // head_size, slot_total, head_size), jnp.float32),
            pltpu.SemaphoreType.DMA((3,)),
        ),
        name="experts",
    )(
        arrived.reshape(lanes, slot_total, share + slab),
        pair_rows,
        expert_gate[0],
        expert_up[0],
        expert_down[0],
    )
    back = exchanged(payload.reshape(devices, capacity, payload_width), EP)
    down_held = lax.all_gather(down_quarter, "zl", axis=1, tiled=False)
    down_all = in_order(down_held[:, None], lax.ppermute(down_held, "c", swap)[:, None], core, 1)
    down_columns = down_all.reshape(width, head_size)
    returned = back[:, :, :width].reshape(slot_total, width)
    dense_parts = back[:, :, width:].reshape(pairs, seq_count, dense_width)
    dense_parts = jnp.sum(dense_parts.astype(jnp.float32), axis=0)
    dense_hidden = jax.nn.silu(dense_parts[:, :head_size]) * dense_parts[:, head_size:]
    dense_terms = product_transposed(dense_hidden.astype(jnp.bfloat16), down_columns)
    side_total = (
        routes[:, 0:1] * product(select_first, returned)
        + routes[:, 1:2] * product(select_second, returned)
        + mix[:, None] * dense_terms
    )
    result = residual.astype(jnp.float32) + summed_over_heads(side_total.astype(jnp.bfloat16))
    return result.astype(jnp.bfloat16)


def solution(mesh):
    chips = mesh.shape["ep"] // 2
    finer = Mesh(mesh.devices.reshape(chips // 4, 4, 2, 4, 4), ("zh", "zl", "c", "y", "x"))
    in_specs = (
        P(EP, None),
        P(),
        P(EP, TP),
        P(EP, TP),
        P(EP, TP),
        P(None, TP),
        P(TP),
        P(EP, TP, None, None),
        P(EP, TP, None, None),
        P(EP, TP, None),
        P(EP),
        P(TP, EP),
        P(),
        P(EP, TP),
        P(EP, TP),
        P(TP, EP),
        P(),
        P(EP, None),
        P(EP),
        P(EP, None),
        P(EP, None, TP),
        P(EP, None, TP),
        P(EP, TP, None),
    )
    out_specs = P(EP, None)
    return jax.shard_map(layer, mesh=finer, in_specs=in_specs, out_specs=out_specs, check_vma=False)
```

```python
import math

import jax
import jax.numpy as jnp
from jax import lax
from jax.experimental import pallas as pl
from jax.experimental.pallas import tpu as pltpu
from jax.sharding import Mesh
from jax.sharding import PartitionSpec as P


EP = ("zh", "zl", "c")
Z = ("zh", "zl")
TP = ("y", "x")
EPSILON = 1e-06


def exchanged(pieces, axes):
    return lax.all_to_all(pieces, axes, split_axis=0, concat_axis=0, tiled=True)


def from_all(array, axis):
    return exchanged(jnp.broadcast_to(array, (lax.axis_size(axis), *array.shape)), axis)


def summed_over_heads(array):
    rows = jnp.sum(from_all(array, "x").astype(jnp.float32), axis=0).astype(jnp.bfloat16)
    return jnp.sum(from_all(rows, "y").astype(jnp.float32), axis=0)


def in_order(own, theirs, place, dim):
    return jnp.where(
        place == 0,
        jnp.concatenate((own, theirs), axis=dim),
        jnp.concatenate((theirs, own), axis=dim),
    )


def product(left, right):
    return jnp.dot(left, right, preferred_element_type=jnp.float32)


def product_transposed(left, right):
    return lax.dot_general(
        left, right, (((1,), (1,)), ((), ())), preferred_element_type=jnp.float32
    )


def rms_scale(values, norm_gain):
    widened = values.astype(jnp.float32)
    return (
        widened
        * lax.rsqrt(jnp.mean(widened * widened, axis=-1, keepdims=True) + EPSILON)
        * norm_gain
    )


def first_payload(
    tokens_ref, gain_ref, out_ref, down_ref, query_ref, key_ref, value_ref, gate_ref, up_ref,
    payload_ref, normed_ref, rows_ref,
):
    seq_count, _ = tokens_ref.shape
    chips, _, slab = payload_ref.shape
    half = seq_count // 2
    held = out_ref.shape[0] // 2
    for k, weight_ref in enumerate((query_ref, key_ref, value_ref, gate_ref, up_ref)):
        rows_ref[:, k * slab : (k + 1) * slab] = weight_ref[...]
    widened = tokens_ref[...].astype(jnp.float32)
    mean = jnp.mean(widened * widened, axis=-1, keepdims=True)
    normed = (widened * lax.rsqrt(mean + EPSILON) * gain_ref[...]).astype(jnp.bfloat16)
    normed_ref[...] = normed
    for chip in range(chips):
        pair, side = divmod(chip, 2)
        for k in range(2):
            first = (2 * pair + k) * slab
            payload_ref[chip, k * half : (k + 1) * half, :] = normed[
                side * half : (side + 1) * half, first : first + slab
            ]
        columns = slice(side * held, (side + 1) * held)
        payload_ref[chip, seq_count : seq_count + held, :] = out_ref[columns, :]
        payload_ref[chip, seq_count + held :, :] = down_ref[columns, :]


def experts(
    rows_ref, dense_ref, gate_hbm, up_hbm, down_hbm, payload_ref,
    gate_ref, up_ref, down_ref, low_ref, high_ref, mixed_ref, sems,
):
    lanes, slots, _ = rows_ref.shape
    width, hidden_width = gate_ref.shape
    share = width // lanes
    slab = dense_ref.shape[0] // 2
    dense_width = hidden_width * 2
    first = dense_ref.shape[1] - dense_width
    copies = [
        pltpu.make_async_copy(source, target, sems.at[k])
        for k, (source, target) in enumerate(
            ((gate_hbm, gate_ref), (up_hbm, up_ref), (down_hbm, down_ref))
        )
    ]
    for copy in copies:
        copy.start()
    for lane in range(lanes):
        pieces = rows_ref[lane, :, share : share + slab]
        low = jnp.dot(pieces, dense_ref[:slab, first:], preferred_element_type=jnp.float32)
        high = jnp.dot(pieces, dense_ref[slab:, first:], preferred_element_type=jnp.float32)
        row, place = divmod(lane, 2)
        for part in range(2):
            span = slice(part * hidden_width, (part + 1) * hidden_width)
            low_ref[part] = low[:, span]
            high_ref[part] = high[:, span]
            mixed_ref[2 * place + part, pl.ds(row, slots // 2, stride=2), :] = (
                low_ref[part, pl.ds(0, slots // 2, stride=2), :]
                + high_ref[part, pl.ds(1, slots // 2, stride=2), :]
            )
    for part in range(mixed_ref.shape[0]):
        span = slice(width + part * hidden_width, width + (part + 1) * hidden_width)
        payload_ref[:, span] = mixed_ref[part].astype(jnp.bfloat16)
    copies[0].wait()
    copies[1].wait()
    gate_part = jnp.zeros((slots, hidden_width), jnp.float32)
    up_part = jnp.zeros((slots, hidden_width), jnp.float32)
    for lane in range(lanes):
        rows = rows_ref[lane, :, :share]
        span = slice(lane * share, (lane + 1) * share)
        gate_part += jnp.dot(rows, gate_ref[span, :], preferred_element_type=jnp.float32)
        up_part += jnp.dot(rows, up_ref[span, :], preferred_element_type=jnp.float32)
    hidden = (gate_part / (1.0 + jnp.exp(-gate_part)) * up_part).astype(jnp.bfloat16)
    copies[2].wait()
    payload_ref[:, :width] = jnp.dot(
        hidden, down_ref[...], preferred_element_type=jnp.float32
    ).astype(jnp.bfloat16)


def attend(queries, keys_new, values_new, key_cache, value_cache, gate_cache, lengths, log_forget):
    cache_span = key_cache.shape[2]
    score_scale = 1.0 / math.sqrt(key_cache.shape[3])
    positions = jnp.arange(cache_span, dtype=jnp.int32)
    live_mask = positions[None, :] < lengths[:, None]
    last_mask = positions[None, :] == lengths[:, None] - 1
    last_gate = jnp.sum(jnp.where(last_mask[:, None, :], gate_cache, 0.0), axis=-1)
    gate_now = last_gate + log_forget
    scores = (
        jnp.einsum("shd,shpd->shp", queries, key_cache, preferred_element_type=jnp.float32)
        * score_scale
    )
    scores = scores + gate_now[:, :, None] - gate_cache
    scores = jnp.where(live_mask[:, None, :], scores, -jnp.inf)
    own_score = (
        jnp.sum(queries.astype(jnp.float32) * keys_new.astype(jnp.float32), axis=-1) * score_scale
    )
    row_top = jnp.maximum(jnp.max(scores, axis=-1), own_score)
    raised = jnp.exp(scores - row_top[:, :, None])
    own_raised = jnp.exp(own_score - row_top)
    totals = jnp.sum(raised, axis=-1) + own_raised
    weights_low = (raised / totals[:, :, None]).astype(jnp.bfloat16)
    own_prob = (own_raised / totals).astype(jnp.bfloat16)
    attended = jnp.einsum(
        "shp,shpd->shd", weights_low, value_cache, preferred_element_type=jnp.float32
    )
    attended = attended + own_prob.astype(jnp.float32)[:, :, None] * values_new.astype(jnp.float32)
    return attended.astype(jnp.bfloat16)


def layer(
    tokens,
    attn_gain,
    query_weight,
    key_weight,
    value_weight,
    forget_weight,
    forget_bias,
    cache_keys,
    cache_values,
    cache_gates,
    lengths,
    output_weight,
    ffn_gain,
    dense_gate_proj,
    dense_up_proj,
    dense_down_proj,
    dense_mix,
    expert_ids,
    group_prob,
    pair_prob,
    expert_gate,
    expert_up,
    expert_down,
):
    seq_count, width = tokens.shape
    head_size = cache_keys.shape[3]
    chips = lax.axis_size(Z)
    quarters = lax.axis_size("zl")
    devices = lax.axis_size(EP)
    slab = width // chips
    core = lax.axis_index("c")
    side = lax.axis_index("zl") % 2
    pairs = chips // 2
    half = seq_count // 2

    held = output_weight.shape[1] // 2
    vmem = pl.BlockSpec(memory_space=pltpu.VMEM)
    payload, normed, own_rows = pl.pallas_call(
        first_payload,
        out_shape=(
            jax.ShapeDtypeStruct((chips, seq_count + 2 * held, slab), jnp.bfloat16),
            jax.ShapeDtypeStruct((seq_count, width), jnp.bfloat16),
            jax.ShapeDtypeStruct((query_weight.shape[0], 5 * slab), jnp.bfloat16),
        ),
        in_specs=(vmem,) * 9,
        out_specs=(vmem,) * 3,
        name="first_payload",
    )(
        tokens,
        attn_gain[None],
        output_weight.T,
        dense_down_proj.T,
        query_weight,
        key_weight,
        value_weight,
        dense_gate_proj,
        dense_up_proj,
    )
    received = exchanged(payload, Z)

    swap = [(0, 1), (1, 0)]
    neighbours = [(k, k ^ 1) for k in range(quarters)]
    their_rows = lax.ppermute(own_rows, "c", swap)
    chip_rows = in_order(own_rows, their_rows, core, 0)
    pair_rows = in_order(chip_rows, lax.ppermute(chip_rows, "zl", neighbours), side, 0)
    projection_width = 3 * head_size
    token_columns = received[:, :seq_count].reshape(chips, 2, half, slab)
    token_columns = token_columns.transpose(0, 2, 1, 3).reshape(chips * half, 2 * slab)

    halves = received[:, seq_count:].reshape(chips, 2, 1, held, slab)
    other_halves = lax.ppermute(halves, "zl", neighbours)
    both = in_order(halves, other_halves, side, 2)
    columns = in_order(both[:, None], lax.ppermute(both, "c", swap)[:, None], core, 1)
    output_columns = columns[:, :, 0].reshape(width, head_size)
    down_columns = columns[:, :, 1].reshape(width, head_size)

    shares = product(token_columns, pair_rows[:, :projection_width]).astype(jnp.bfloat16)
    shares = exchanged(shares.reshape(chips, half, projection_width), Z)
    shares = shares.reshape(pairs, seq_count, projection_width)
    projected = jnp.sum(shares.astype(jnp.float32), axis=0).astype(jnp.bfloat16)
    projected = projected.reshape(seq_count, 3, 1, head_size)
    log_forget = jax.nn.log_sigmoid(product(normed, forget_weight) + forget_bias)
    attended = attend(
        projected[:, 0],
        projected[:, 1],
        projected[:, 2],
        cache_keys,
        cache_values,
        cache_gates,
        lengths,
        log_forget,
    ).reshape(seq_count, head_size)
    picks = expert_ids.reshape(-1)
    capacity = 4 * seq_count // devices
    slot_total = devices * capacity
    pick_onehot = (picks[:, None] == jnp.arange(devices, dtype=jnp.int32)[None, :]).astype(jnp.int32)
    earlier = jnp.cumsum(pick_onehot, axis=0) - pick_onehot
    slot_rank = jnp.sum(earlier * pick_onehot, axis=1)
    destination = (picks * capacity + slot_rank).reshape(seq_count, 2)
    slot_grid = jnp.arange(slot_total, dtype=jnp.int32)
    select_first = (destination[:, 0:1] == slot_grid[None, :]).astype(jnp.bfloat16)
    select_second = (destination[:, 1:2] == slot_grid[None, :]).astype(jnp.bfloat16)
    routes = group_prob[:, None] * pair_prob / jnp.sum(pair_prob, axis=1, keepdims=True)
    head_terms = product_transposed(attended, output_columns).astype(jnp.bfloat16)
    lane = lax.axis_index("x")
    share = width // lax.axis_size("x")
    head_terms, selectors, routes, lane, share_start, mix_row = lax.optimization_barrier(
        (
            head_terms,
            (select_first, select_second),
            (routes[:, 0], routes[:, 1]),
            lane,
            lane * share,
            dense_mix.astype(jnp.float32),
        )
    )
    select_first, select_second = selectors
    residual = (tokens.astype(jnp.float32) + summed_over_heads(head_terms)).astype(jnp.bfloat16)
    ffn_in = rms_scale(residual, ffn_gain).astype(jnp.bfloat16)
    mix = jax.nn.sigmoid(jnp.sum(ffn_in.astype(jnp.float32) * mix_row, axis=-1))

    lanes = lax.axis_size("x")
    ffn_share = lax.dynamic_slice_in_dim(
        ffn_in, share_start, share, axis=1, allow_negative_indices=False
    )
    outbound = jnp.einsum(
        "sk,sd->kd", select_first + select_second, ffn_share, preferred_element_type=jnp.float32
    )
    outbound = outbound.astype(jnp.bfloat16).reshape(devices, capacity, share)
    few = seq_count // 4
    dense_pieces = ffn_in.reshape(4, few, pairs, 2, slab)
    dense_pieces = lax.dynamic_index_in_dim(
        dense_pieces, lane, axis=1, keepdims=False, allow_negative_indices=False
    )
    dense_pieces = dense_pieces.transpose(1, 0, 2, 3).reshape(devices, 2, slab)
    outbound, mix = lax.optimization_barrier(
        (jnp.concatenate((outbound, dense_pieces), axis=2), mix)
    )
    arrived = exchanged(outbound, EP)
    arrived = from_all(arrived, "x")
    dense_width = 2 * head_size
    payload_width = width + few // capacity * dense_width
    hbm = pl.BlockSpec(memory_space=pl.ANY)
    payload = pl.pallas_call(
        experts,
        out_shape=jax.ShapeDtypeStruct((slot_total, payload_width), jnp.bfloat16),
        in_specs=(vmem, vmem, hbm, hbm, hbm),
        out_specs=vmem,
        scratch_shapes=(
            pltpu.VMEM(expert_gate.shape[1:], jnp.bfloat16),
            pltpu.VMEM(expert_up.shape[1:], jnp.bfloat16),
            pltpu.VMEM(expert_down.shape[1:], jnp.bfloat16),
            pltpu.VMEM((2, slot_total, head_size), jnp.float32),
            pltpu.VMEM((2, slot_total, head_size), jnp.float32),
            pltpu.VMEM(((payload_width - width) // head_size, slot_total, head_size), jnp.float32),
            pltpu.SemaphoreType.DMA((3,)),
        ),
        name="experts",
    )(
        arrived.reshape(lanes, slot_total, share + slab),
        pair_rows,
        expert_gate[0],
        expert_up[0],
        expert_down[0],
    )
    back = exchanged(payload.reshape(devices, capacity, payload_width), EP)
    returned = back[:, :, :width].reshape(slot_total, width)
    dense_parts = back[:, :, width:].reshape(pairs, seq_count, dense_width)
    dense_parts = jnp.sum(dense_parts.astype(jnp.float32), axis=0)
    dense_hidden = jax.nn.silu(dense_parts[:, :head_size]) * dense_parts[:, head_size:]
    dense_terms = product_transposed(dense_hidden.astype(jnp.bfloat16), down_columns)
    side_total = (
        routes[0][:, None] * product(select_first, returned)
        + routes[1][:, None] * product(select_second, returned)
        + mix[:, None] * dense_terms
    )
    result = residual.astype(jnp.float32) + summed_over_heads(side_total.astype(jnp.bfloat16))
    return result.astype(jnp.bfloat16)


def solution(mesh):
    chips = mesh.shape["ep"] // 2
    finer = Mesh(mesh.devices.reshape(chips // 4, 4, 2, 4, 4), ("zh", "zl", "c", "y", "x"))
    in_specs = (
        P(EP, None),
        P(),
        P(EP, TP),
        P(EP, TP),
        P(EP, TP),
        P(None, TP),
        P(TP),
        P(EP, TP, None, None),
        P(EP, TP, None, None),
        P(EP, TP, None),
        P(EP),
        P(TP, EP),
        P(),
        P(EP, TP),
        P(EP, TP),
        P(TP, EP),
        P(),
        P(EP, None),
        P(EP),
        P(EP, None),
        P(EP, None, TP),
        P(EP, None, TP),
        P(EP, TP, None),
    )
    out_specs = P(EP, None)
    return jax.shard_map(layer, mesh=finer, in_specs=in_specs, out_specs=out_specs, check_vma=False)
```

```python
import math

import jax
import jax.numpy as jnp
from jax import lax
from jax.experimental import pallas as pl
from jax.experimental.pallas import tpu as pltpu
from jax.sharding import Mesh
from jax.sharding import PartitionSpec as P


EP = ("zh", "zl", "c")
Z = ("zh", "zl")
TP = ("y", "x")
EPSILON = 1e-06


def exchanged(pieces, axes):
    return lax.all_to_all(pieces, axes, split_axis=0, concat_axis=0, tiled=True)


def from_all(array, axis):
    return exchanged(jnp.broadcast_to(array, (lax.axis_size(axis), *array.shape)), axis)


def summed_over_heads(array):
    rows = jnp.sum(from_all(array, "x").astype(jnp.float32), axis=0).astype(jnp.bfloat16)
    return jnp.sum(from_all(rows, "y").astype(jnp.float32), axis=0)


def in_order(own, theirs, place, dim):
    return jnp.where(
        place == 0,
        jnp.concatenate((own, theirs), axis=dim),
        jnp.concatenate((theirs, own), axis=dim),
    )


def product(left, right):
    return jnp.dot(left, right, preferred_element_type=jnp.float32)


def product_transposed(left, right):
    return lax.dot_general(
        left, right, (((1,), (1,)), ((), ())), preferred_element_type=jnp.float32
    )


def rms_scale(values, norm_gain):
    widened = values.astype(jnp.float32)
    return (
        widened
        * lax.rsqrt(jnp.mean(widened * widened, axis=-1, keepdims=True) + EPSILON)
        * norm_gain
    )


def first_payload(
    tokens_ref, gain_ref, out_ref, down_ref, query_ref, key_ref, value_ref, gate_ref, up_ref,
    forget_ref, bias_ref, ids_ref, pair_ref, group_ref,
    payload_ref, logits_ref, rows_ref, first_ref, second_ref, routes_ref,
):
    seq_count, _ = tokens_ref.shape
    chips, _, slab = payload_ref.shape
    held = out_ref.shape[0] // 2
    for k, weight_ref in enumerate((query_ref, key_ref, value_ref, gate_ref, up_ref)):
        rows_ref[:, k * slab : (k + 1) * slab] = weight_ref[...]
    widened = tokens_ref[...].astype(jnp.float32)
    mean = jnp.mean(widened * widened, axis=-1, keepdims=True)
    normed = (widened * lax.rsqrt(mean + EPSILON) * gain_ref[...]).astype(jnp.bfloat16)
    forget = normed.astype(jnp.float32) * forget_ref[...].astype(jnp.float32)
    logits_ref[...] = jnp.sum(forget, axis=-1, keepdims=True) + bias_ref[...]
    for chip in range(chips):
        side = chip % 2
        payload_ref[chip, :seq_count, :] = normed[:, chip * slab : (chip + 1) * slab]
        columns = slice(side * held, (side + 1) * held)
        payload_ref[chip, seq_count : seq_count + held, :] = out_ref[columns, :]
        payload_ref[chip, seq_count + held :, :] = down_ref[columns, :]

    row = lax.broadcasted_iota(jnp.int32, (seq_count, seq_count), 0)
    place = lax.broadcasted_iota(jnp.int32, (seq_count, seq_count), 1)

    def column(values):
        return jnp.sum(jnp.where(row == place, values, 0.0), axis=1, keepdims=True)

    slot_total = first_ref.shape[1]
    devices = 2 * chips
    grid = lax.broadcasted_iota(jnp.int32, (seq_count, devices), 1).astype(jnp.float32)
    slots = lax.broadcasted_iota(jnp.int32, (seq_count, slot_total), 1).astype(jnp.float32)
    named = [column(ids_ref[k : k + 1, :].astype(jnp.float32)) for k in range(2)]
    hot = [(expert == grid).astype(jnp.float32) for expert in named]
    before = jnp.dot(
        (place < row).astype(jnp.float32), hot[0] + hot[1], preferred_element_type=jnp.float32
    )
    for k, select_ref in enumerate((first_ref, second_ref)):
        rank = jnp.sum(before * hot[k], axis=1, keepdims=True)
        target = named[k] * (slot_total // devices) + rank
        select_ref[...] = (target == slots).astype(jnp.float32).astype(jnp.bfloat16)
    pair = [column(pair_ref[k : k + 1, :]) for k in range(2)]
    group = column(group_ref[...])
    for k in range(2):
        routes_ref[k] = group * pair[k] / (pair[0] + pair[1])


def experts(
    rows_ref, dense_ref, gate_hbm, up_hbm, down_hbm, payload_ref,
    gate_ref, up_ref, down_ref, sems,
):
    lanes, slots, _ = rows_ref.shape
    width, hidden_width = gate_ref.shape
    share = width // lanes
    slab = dense_ref.shape[0]
    dense_width = hidden_width * 2
    first = dense_ref.shape[1] - dense_width
    copies = [
        pltpu.make_async_copy(source, target, sems.at[k])
        for k, (source, target) in enumerate(
            ((gate_hbm, gate_ref), (up_hbm, up_ref), (down_hbm, down_ref))
        )
    ]
    for copy in copies:
        copy.start()
    for lane in range(lanes):
        start = width + lane * dense_width
        payload_ref[:, start : start + dense_width] = jnp.dot(
            rows_ref[lane, :, share : share + slab],
            dense_ref[:, first:],
            preferred_element_type=jnp.float32,
        ).astype(jnp.bfloat16)
    copies[0].wait()
    copies[1].wait()
    gate_part = jnp.zeros((slots, hidden_width), jnp.float32)
    up_part = jnp.zeros((slots, hidden_width), jnp.float32)
    for lane in range(lanes):
        rows = rows_ref[lane, :, :share]
        span = slice(lane * share, (lane + 1) * share)
        gate_part += jnp.dot(rows, gate_ref[span, :], preferred_element_type=jnp.float32)
        up_part += jnp.dot(rows, up_ref[span, :], preferred_element_type=jnp.float32)
    hidden = (gate_part / (1.0 + jnp.exp(-gate_part)) * up_part).astype(jnp.bfloat16)
    copies[2].wait()
    payload_ref[:, :width] = jnp.dot(
        hidden, down_ref[...], preferred_element_type=jnp.float32
    ).astype(jnp.bfloat16)


def attend(queries, keys_new, values_new, key_cache, value_cache, gate_cache, lengths, log_forget):
    cache_span = key_cache.shape[2]
    score_scale = 1.0 / math.sqrt(key_cache.shape[3])
    positions = jnp.arange(cache_span, dtype=jnp.int32)
    live_mask = positions[None, :] < lengths[:, None]
    last_mask = positions[None, :] == lengths[:, None] - 1
    last_gate = jnp.sum(jnp.where(last_mask[:, None, :], gate_cache, 0.0), axis=-1)
    gate_now = last_gate + log_forget
    scores = (
        jnp.einsum("shd,shpd->shp", queries, key_cache, preferred_element_type=jnp.float32)
        * score_scale
    )
    scores = scores + gate_now[:, :, None] - gate_cache
    scores = jnp.where(live_mask[:, None, :], scores, -jnp.inf)
    own_score = (
        jnp.sum(queries.astype(jnp.float32) * keys_new.astype(jnp.float32), axis=-1) * score_scale
    )
    row_top = jnp.maximum(jnp.max(scores, axis=-1), own_score)
    raised = jnp.exp(scores - row_top[:, :, None])
    own_raised = jnp.exp(own_score - row_top)
    totals = jnp.sum(raised, axis=-1) + own_raised
    weights_low = (raised / totals[:, :, None]).astype(jnp.bfloat16)
    own_prob = (own_raised / totals).astype(jnp.bfloat16)
    attended = jnp.einsum(
        "shp,shpd->shd", weights_low, value_cache, preferred_element_type=jnp.float32
    )
    attended = attended + own_prob.astype(jnp.float32)[:, :, None] * values_new.astype(jnp.float32)
    return attended.astype(jnp.bfloat16)


def layer(
    tokens,
    attn_gain,
    query_weight,
    key_weight,
    value_weight,
    forget_weight,
    forget_bias,
    cache_keys,
    cache_values,
    cache_gates,
    lengths,
    output_weight,
    ffn_gain,
    dense_gate_proj,
    dense_up_proj,
    dense_down_proj,
    dense_mix,
    expert_ids,
    group_prob,
    pair_prob,
    expert_gate,
    expert_up,
    expert_down,
):
    seq_count, width = tokens.shape
    head_size = cache_keys.shape[3]
    chips = lax.axis_size(Z)
    quarters = lax.axis_size("zl")
    devices = lax.axis_size(EP)
    slab = width // chips
    core = lax.axis_index("c")
    side = lax.axis_index("zl") % 2

    held = output_weight.shape[1] // 2
    vmem = pl.BlockSpec(memory_space=pltpu.VMEM)
    capacity = 4 * seq_count // devices
    slot_total = devices * capacity
    payload, forget_logits, own_rows, *routing = pl.pallas_call(
        first_payload,
        out_shape=(
            pltpu.VMEM((chips, seq_count + 2 * held, slab), jnp.bfloat16),
            jax.ShapeDtypeStruct((seq_count, 1), jnp.float32),
            jax.ShapeDtypeStruct((query_weight.shape[0], 5 * slab), jnp.bfloat16),
            jax.ShapeDtypeStruct((seq_count, slot_total), jnp.bfloat16),
            jax.ShapeDtypeStruct((seq_count, slot_total), jnp.bfloat16),
            jax.ShapeDtypeStruct((2, seq_count, 1), jnp.float32),
        ),
        in_specs=(vmem,) * 14,
        out_specs=(vmem,) * 6,
        name="first_payload",
    )(
        tokens,
        attn_gain[None],
        output_weight.T,
        dense_down_proj.T,
        query_weight,
        key_weight,
        value_weight,
        dense_gate_proj,
        dense_up_proj,
        forget_weight.T,
        forget_bias[None],
        expert_ids.T,
        pair_prob.T,
        group_prob[None],
    )
    select_first, select_second, routes = routing
    swap = [(0, 1), (1, 0)]
    neighbours = [(k, k ^ 1) for k in range(quarters)]
    their_rows = lax.ppermute(own_rows, "c", swap)
    payload, their_rows, core, side, lane = lax.optimization_barrier(
        (payload, their_rows, core, side, lax.axis_index("x"))
    )
    received = exchanged(payload, Z)
    (
        received, their_rows, own_rows, forget_logits, cache_gates, lengths, select_first,
        select_second, routes, dense_mix, core, side, lane,
    ) = lax.optimization_barrier(
        (
            received, their_rows, own_rows, forget_logits, cache_gates, lengths, select_first,
            select_second, routes, dense_mix, core, side, lane,
        )
    )
    chip_rows = in_order(own_rows, their_rows, core, 0)
    projection_width = 3 * head_size
    token_columns = received[:, :seq_count].reshape(chips * seq_count, slab)

    halves = received[:, seq_count:].reshape(chips, 2, 1, held, slab)
    other_halves = lax.ppermute(halves, "zl", neighbours)
    both = in_order(halves, other_halves, side, 2)
    columns = in_order(both[:, None], lax.ppermute(both, "c", swap)[:, None], core, 1)
    output_columns = columns[:, :, 0].reshape(width, head_size)
    down_columns = columns[:, :, 1].reshape(width, head_size)

    shares = product(token_columns, chip_rows[:, :projection_width]).astype(jnp.bfloat16)
    shares = exchanged(shares.reshape(chips, seq_count, projection_width), Z)
    projected = jnp.sum(shares.astype(jnp.float32), axis=0).astype(jnp.bfloat16)
    projected = projected.reshape(seq_count, 3, 1, head_size)
    log_forget = jax.nn.log_sigmoid(forget_logits)
    attended = attend(
        projected[:, 0],
        projected[:, 1],
        projected[:, 2],
        cache_keys,
        cache_values,
        cache_gates,
        lengths,
        log_forget,
    ).reshape(seq_count, head_size)
    head_terms = product_transposed(attended, output_columns).astype(jnp.bfloat16)
    share = width // lax.axis_size("x")
    head_terms, selectors, routes, lane, share_start, mix_row = lax.optimization_barrier(
        (
            head_terms,
            (select_first, select_second),
            (routes[0], routes[1]),
            lane,
            lane * share,
            dense_mix.astype(jnp.float32),
        )
    )
    select_first, select_second = selectors
    residual = (tokens.astype(jnp.float32) + summed_over_heads(head_terms)).astype(jnp.bfloat16)
    ffn_in = rms_scale(residual, ffn_gain).astype(jnp.bfloat16)
    mix = jax.nn.sigmoid(jnp.sum(ffn_in.astype(jnp.float32) * mix_row, axis=-1))

    lanes = lax.axis_size("x")
    ffn_share = lax.dynamic_slice_in_dim(
        ffn_in, share_start, share, axis=1, allow_negative_indices=False
    )
    outbound = jnp.einsum(
        "sk,sd->kd", select_first + select_second, ffn_share, preferred_element_type=jnp.float32
    )
    outbound = outbound.astype(jnp.bfloat16).reshape(devices, capacity, share)
    dense_pieces = ffn_in.reshape(2, capacity, lanes, chips, slab)
    dense_pieces = lax.dynamic_index_in_dim(
        dense_pieces, lane, axis=2, keepdims=False, allow_negative_indices=False
    )
    dense_pieces = dense_pieces.transpose(2, 0, 1, 3).reshape(devices, capacity, slab)
    outbound, mix = lax.optimization_barrier(
        (jnp.concatenate((outbound, dense_pieces), axis=2), mix)
    )
    arrived = exchanged(outbound, EP)
    arrived = from_all(arrived, "x")
    dense_width = 2 * head_size
    payload_width = width + lanes * dense_width
    hbm = pl.BlockSpec(memory_space=pl.ANY)
    payload = pl.pallas_call(
        experts,
        out_shape=pltpu.VMEM((slot_total, payload_width), jnp.bfloat16),
        in_specs=(vmem, vmem, hbm, hbm, hbm),
        out_specs=vmem,
        scratch_shapes=(
            pltpu.VMEM(expert_gate.shape[1:], jnp.bfloat16),
            pltpu.VMEM(expert_up.shape[1:], jnp.bfloat16),
            pltpu.VMEM(expert_down.shape[1:], jnp.bfloat16),
            pltpu.SemaphoreType.DMA((3,)),
        ),
        name="experts",
    )(
        arrived.reshape(lanes, slot_total, share + slab),
        chip_rows,
        expert_gate[0],
        expert_up[0],
        expert_down[0],
    )
    back = exchanged(payload.reshape(devices, capacity, payload_width), EP)
    returned = back[:, :, :width].reshape(slot_total, width)
    dense_parts = back[:, :, width:].reshape(chips, seq_count, dense_width)
    dense_parts = jnp.sum(dense_parts.astype(jnp.float32), axis=0)
    dense_hidden = jax.nn.silu(dense_parts[:, :head_size]) * dense_parts[:, head_size:]
    dense_terms = product_transposed(dense_hidden.astype(jnp.bfloat16), down_columns)
    side_total = (
        routes[0] * product(select_first, returned)
        + routes[1] * product(select_second, returned)
        + mix[:, None] * dense_terms
    )
    result = residual.astype(jnp.float32) + summed_over_heads(side_total.astype(jnp.bfloat16))
    return result.astype(jnp.bfloat16)


def solution(mesh):
    chips = mesh.shape["ep"] // 2
    finer = Mesh(mesh.devices.reshape(chips // 4, 4, 2, 4, 4), ("zh", "zl", "c", "y", "x"))
    in_specs = (
        P(EP, None),
        P(),
        P(EP, TP),
        P(EP, TP),
        P(EP, TP),
        P(None, TP),
        P(TP),
        P(EP, TP, None, None),
        P(EP, TP, None, None),
        P(EP, TP, None),
        P(EP),
        P(TP, EP),
        P(),
        P(EP, TP),
        P(EP, TP),
        P(TP, EP),
        P(),
        P(EP, None),
        P(EP),
        P(EP, None),
        P(EP, None, TP),
        P(EP, None, TP),
        P(EP, TP, None),
    )
    out_specs = P(EP, None)
    return jax.shard_map(layer, mesh=finer, in_specs=in_specs, out_specs=out_specs, check_vma=False)
```

```python
import math

import jax
import jax.numpy as jnp
from jax import lax
from jax.experimental import pallas as pl
from jax.experimental.pallas import tpu as pltpu
from jax.sharding import Mesh
from jax.sharding import PartitionSpec as P


EP = ("zh", "zl", "c")
Z = ("zh", "zl")
TP = ("y", "x")
EPSILON = 1e-06


def exchanged(pieces, axes):
    return lax.all_to_all(pieces, axes, split_axis=0, concat_axis=0, tiled=True)


def from_all(array, axis):
    return exchanged(jnp.broadcast_to(array, (lax.axis_size(axis), *array.shape)), axis)


def summed_over_heads(array):
    rows = jnp.sum(from_all(array, "x").astype(jnp.float32), axis=0).astype(jnp.bfloat16)
    return jnp.sum(from_all(rows, "y").astype(jnp.float32), axis=0)


def in_order(own, theirs, place, dim):
    return jnp.where(
        place == 0,
        jnp.concatenate((own, theirs), axis=dim),
        jnp.concatenate((theirs, own), axis=dim),
    )


def product(left, right):
    return jnp.dot(left, right, preferred_element_type=jnp.float32)


def product_transposed(left, right):
    return lax.dot_general(
        left, right, (((1,), (1,)), ((), ())), preferred_element_type=jnp.float32
    )


def rms_scale(values, norm_gain):
    widened = values.astype(jnp.float32)
    return (
        widened
        * lax.rsqrt(jnp.mean(widened * widened, axis=-1, keepdims=True) + EPSILON)
        * norm_gain
    )


def first_payload(
    tokens_ref, gain_ref, out_ref, down_ref, query_ref, key_ref, value_ref, gate_ref, up_ref,
    forget_ref, bias_ref, ids_ref, pair_ref, group_ref,
    payload_ref, logits_ref, rows_ref, first_ref, second_ref, routes_ref,
):
    seq_count, _ = tokens_ref.shape
    chips, _, slab = payload_ref.shape
    half = seq_count // 2
    held = out_ref.shape[0] // 2
    for k, weight_ref in enumerate((query_ref, key_ref, value_ref, gate_ref, up_ref)):
        rows_ref[:, k * slab : (k + 1) * slab] = weight_ref[...]
    widened = tokens_ref[...].astype(jnp.float32)
    mean = jnp.mean(widened * widened, axis=-1, keepdims=True)
    normed = (widened * lax.rsqrt(mean + EPSILON) * gain_ref[...]).astype(jnp.bfloat16)
    forget = normed.astype(jnp.float32) * forget_ref[...].astype(jnp.float32)
    logits_ref[...] = jnp.sum(forget, axis=-1, keepdims=True) + bias_ref[...]
    for chip in range(chips):
        pair, side = divmod(chip, 2)
        for k in range(2):
            first = (2 * pair + k) * slab
            payload_ref[chip, k * half : (k + 1) * half, :] = normed[
                side * half : (side + 1) * half, first : first + slab
            ]
        columns = slice(side * held, (side + 1) * held)
        payload_ref[chip, seq_count : seq_count + held, :] = out_ref[columns, :]
        payload_ref[chip, seq_count + held :, :] = down_ref[columns, :]

    row = lax.broadcasted_iota(jnp.int32, (seq_count, seq_count), 0)
    place = lax.broadcasted_iota(jnp.int32, (seq_count, seq_count), 1)

    def column(values):
        return jnp.sum(jnp.where(row == place, values, 0.0), axis=1, keepdims=True)

    slot_total = first_ref.shape[1]
    devices = 2 * chips
    grid = lax.broadcasted_iota(jnp.int32, (seq_count, devices), 1).astype(jnp.float32)
    slots = lax.broadcasted_iota(jnp.int32, (seq_count, slot_total), 1).astype(jnp.float32)
    named = [column(ids_ref[k : k + 1, :].astype(jnp.float32)) for k in range(2)]
    hot = [(expert == grid).astype(jnp.float32) for expert in named]
    before = jnp.dot(
        (place < row).astype(jnp.float32), hot[0] + hot[1], preferred_element_type=jnp.float32
    )
    for k, select_ref in enumerate((first_ref, second_ref)):
        rank = jnp.sum(before * hot[k], axis=1, keepdims=True)
        target = named[k] * (slot_total // devices) + rank
        select_ref[...] = (target == slots).astype(jnp.float32).astype(jnp.bfloat16)
    odds = [column(pair_ref[k : k + 1, :]) for k in range(2)]
    group = column(group_ref[...])
    for k in range(2):
        routes_ref[k] = group * odds[k] / (odds[0] + odds[1])


def experts(
    rows_ref, dense_ref, gate_hbm, up_hbm, down_hbm, payload_ref,
    gate_ref, up_ref, down_ref, low_ref, high_ref, mixed_ref, sems,
):
    lanes, slots, _ = rows_ref.shape
    width, hidden_width = gate_ref.shape
    share = width // lanes
    slab = dense_ref.shape[0] // 2
    dense_width = hidden_width * 2
    first = dense_ref.shape[1] - dense_width
    copies = [
        pltpu.make_async_copy(source, target, sems.at[k])
        for k, (source, target) in enumerate(
            ((gate_hbm, gate_ref), (up_hbm, up_ref), (down_hbm, down_ref))
        )
    ]
    for copy in copies:
        copy.start()
    for lane in range(lanes):
        pieces = rows_ref[lane, :, share : share + slab]
        low = jnp.dot(pieces, dense_ref[:slab, first:], preferred_element_type=jnp.float32)
        high = jnp.dot(pieces, dense_ref[slab:, first:], preferred_element_type=jnp.float32)
        row, place = divmod(lane, 2)
        for part in range(2):
            span = slice(part * hidden_width, (part + 1) * hidden_width)
            low_ref[part] = low[:, span]
            high_ref[part] = high[:, span]
            mixed_ref[2 * place + part, pl.ds(row, slots // 2, stride=2), :] = (
                low_ref[part, pl.ds(0, slots // 2, stride=2), :]
                + high_ref[part, pl.ds(1, slots // 2, stride=2), :]
            )
    for part in range(mixed_ref.shape[0]):
        span = slice(width + part * hidden_width, width + (part + 1) * hidden_width)
        payload_ref[:, span] = mixed_ref[part].astype(jnp.bfloat16)
    copies[0].wait()
    copies[1].wait()
    gate_part = jnp.zeros((slots, hidden_width), jnp.float32)
    up_part = jnp.zeros((slots, hidden_width), jnp.float32)
    for lane in range(lanes):
        rows = rows_ref[lane, :, :share]
        span = slice(lane * share, (lane + 1) * share)
        gate_part += jnp.dot(rows, gate_ref[span, :], preferred_element_type=jnp.float32)
        up_part += jnp.dot(rows, up_ref[span, :], preferred_element_type=jnp.float32)
    hidden = (gate_part / (1.0 + jnp.exp(-gate_part)) * up_part).astype(jnp.bfloat16)
    copies[2].wait()
    payload_ref[:, :width] = jnp.dot(
        hidden, down_ref[...], preferred_element_type=jnp.float32
    ).astype(jnp.bfloat16)


def attend(queries, keys_new, values_new, key_cache, value_cache, gate_cache, lengths, log_forget):
    cache_span = key_cache.shape[2]
    score_scale = 1.0 / math.sqrt(key_cache.shape[3])
    positions = jnp.arange(cache_span, dtype=jnp.int32)
    live_mask = positions[None, :] < lengths[:, None]
    last_mask = positions[None, :] == lengths[:, None] - 1
    last_gate = jnp.sum(jnp.where(last_mask[:, None, :], gate_cache, 0.0), axis=-1)
    gate_now = last_gate + log_forget
    scores = (
        jnp.einsum("shd,shpd->shp", queries, key_cache, preferred_element_type=jnp.float32)
        * score_scale
    )
    scores = scores + gate_now[:, :, None] - gate_cache
    scores = jnp.where(live_mask[:, None, :], scores, -jnp.inf)
    own_score = (
        jnp.sum(queries.astype(jnp.float32) * keys_new.astype(jnp.float32), axis=-1) * score_scale
    )
    row_top = jnp.maximum(jnp.max(scores, axis=-1), own_score)
    raised = jnp.exp(scores - row_top[:, :, None])
    own_raised = jnp.exp(own_score - row_top)
    totals = jnp.sum(raised, axis=-1) + own_raised
    weights_low = (raised / totals[:, :, None]).astype(jnp.bfloat16)
    own_prob = (own_raised / totals).astype(jnp.bfloat16)
    attended = jnp.einsum(
        "shp,shpd->shd", weights_low, value_cache, preferred_element_type=jnp.float32
    )
    attended = attended + own_prob.astype(jnp.float32)[:, :, None] * values_new.astype(jnp.float32)
    return attended.astype(jnp.bfloat16)


def layer(
    tokens,
    attn_gain,
    query_weight,
    key_weight,
    value_weight,
    forget_weight,
    forget_bias,
    cache_keys,
    cache_values,
    cache_gates,
    lengths,
    output_weight,
    ffn_gain,
    dense_gate_proj,
    dense_up_proj,
    dense_down_proj,
    dense_mix,
    expert_ids,
    group_prob,
    pair_prob,
    expert_gate,
    expert_up,
    expert_down,
):
    seq_count, width = tokens.shape
    head_size = cache_keys.shape[3]
    chips = lax.axis_size(Z)
    quarters = lax.axis_size("zl")
    devices = lax.axis_size(EP)
    slab = width // chips
    core = lax.axis_index("c")
    side = lax.axis_index("zl") % 2
    pairs = chips // 2
    half = seq_count // 2

    held = output_weight.shape[1] // 2
    vmem = pl.BlockSpec(memory_space=pltpu.VMEM)
    capacity = 4 * seq_count // devices
    slot_total = devices * capacity
    payload, forget_logits, own_rows, *routing = pl.pallas_call(
        first_payload,
        out_shape=(
            jax.ShapeDtypeStruct((chips, seq_count + 2 * held, slab), jnp.bfloat16),
            jax.ShapeDtypeStruct((seq_count, 1), jnp.float32),
            pltpu.VMEM((query_weight.shape[0], 5 * slab), jnp.bfloat16),
            jax.ShapeDtypeStruct((seq_count, slot_total), jnp.bfloat16),
            jax.ShapeDtypeStruct((seq_count, slot_total), jnp.bfloat16),
            jax.ShapeDtypeStruct((2, seq_count, 1), jnp.float32),
        ),
        in_specs=(vmem,) * 14,
        out_specs=(vmem,) * 6,
        name="first_payload",
    )(
        tokens,
        attn_gain[None],
        output_weight.T,
        dense_down_proj.T,
        query_weight,
        key_weight,
        value_weight,
        dense_gate_proj,
        dense_up_proj,
        forget_weight.T,
        forget_bias[None],
        expert_ids.T,
        pair_prob.T,
        group_prob[None],
    )
    select_first, select_second, routes = routing
    received = exchanged(payload, Z)

    swap = [(0, 1), (1, 0)]
    neighbours = [(k, k ^ 1) for k in range(quarters)]
    their_rows = lax.ppermute(own_rows, "c", swap)
    chip_rows = in_order(own_rows, their_rows, core, 0)
    pair_rows = in_order(chip_rows, lax.ppermute(chip_rows, "zl", neighbours), side, 0)
    projection_width = 3 * head_size
    token_columns = received[:, :seq_count].reshape(chips, 2, half, slab)
    token_columns = token_columns.transpose(0, 2, 1, 3).reshape(chips * half, 2 * slab)

    halves = received[:, seq_count:].reshape(chips, 2, 1, held, slab)
    other_halves = lax.ppermute(halves, "zl", neighbours)
    both = in_order(halves, other_halves, side, 2)
    columns = in_order(both[:, None], lax.ppermute(both, "c", swap)[:, None], core, 1)
    output_columns = columns[:, :, 0].reshape(width, head_size)
    down_columns = columns[:, :, 1].reshape(width, head_size)

    shares = product(token_columns, pair_rows[:, :projection_width]).astype(jnp.bfloat16)
    shares = exchanged(shares.reshape(chips, half, projection_width), Z)
    shares = shares.reshape(pairs, seq_count, projection_width)
    projected = jnp.sum(shares.astype(jnp.float32), axis=0).astype(jnp.bfloat16)
    projected = projected.reshape(seq_count, 3, 1, head_size)
    log_forget = jax.nn.log_sigmoid(forget_logits)
    attended = attend(
        projected[:, 0],
        projected[:, 1],
        projected[:, 2],
        cache_keys,
        cache_values,
        cache_gates,
        lengths,
        log_forget,
    ).reshape(seq_count, head_size)
    head_terms = product_transposed(attended, output_columns).astype(jnp.bfloat16)
    lane = lax.axis_index("x")
    share = width // lax.axis_size("x")
    head_terms, selectors, routes, lane, share_start, mix_row = lax.optimization_barrier(
        (
            head_terms,
            (select_first, select_second),
            (routes[0], routes[1]),
            lane,
            lane * share,
            dense_mix.astype(jnp.float32),
        )
    )
    select_first, select_second = selectors
    residual = (tokens.astype(jnp.float32) + summed_over_heads(head_terms)).astype(jnp.bfloat16)
    ffn_in = rms_scale(residual, ffn_gain).astype(jnp.bfloat16)
    mix = jax.nn.sigmoid(jnp.sum(ffn_in.astype(jnp.float32) * mix_row, axis=-1))

    lanes = lax.axis_size("x")
    ffn_share = lax.dynamic_slice_in_dim(
        ffn_in, share_start, share, axis=1, allow_negative_indices=False
    )
    outbound = jnp.einsum(
        "sk,sd->kd", select_first + select_second, ffn_share, preferred_element_type=jnp.float32
    )
    outbound = outbound.astype(jnp.bfloat16).reshape(devices, capacity, share)
    few = seq_count // 4
    dense_pieces = ffn_in.reshape(4, few, pairs, 2, slab)
    dense_pieces = lax.dynamic_index_in_dim(
        dense_pieces, lane, axis=1, keepdims=False, allow_negative_indices=False
    )
    dense_pieces = dense_pieces.transpose(1, 0, 2, 3).reshape(devices, 2, slab)
    outbound, mix = lax.optimization_barrier(
        (jnp.concatenate((outbound, dense_pieces), axis=2), mix)
    )
    arrived = exchanged(outbound, EP)
    arrived = from_all(arrived, "x")
    dense_width = 2 * head_size
    payload_width = width + few // capacity * dense_width
    hbm = pl.BlockSpec(memory_space=pl.ANY)
    payload = pl.pallas_call(
        experts,
        out_shape=pltpu.VMEM((slot_total, payload_width), jnp.bfloat16),
        in_specs=(vmem, vmem, hbm, hbm, hbm),
        out_specs=vmem,
        scratch_shapes=(
            pltpu.VMEM(expert_gate.shape[1:], jnp.bfloat16),
            pltpu.VMEM(expert_up.shape[1:], jnp.bfloat16),
            pltpu.VMEM(expert_down.shape[1:], jnp.bfloat16),
            pltpu.VMEM((2, slot_total, head_size), jnp.float32),
            pltpu.VMEM((2, slot_total, head_size), jnp.float32),
            pltpu.VMEM(((payload_width - width) // head_size, slot_total, head_size), jnp.float32),
            pltpu.SemaphoreType.DMA((3,)),
        ),
        name="experts",
    )(
        arrived.reshape(lanes, slot_total, share + slab),
        pair_rows,
        expert_gate[0],
        expert_up[0],
        expert_down[0],
    )
    back = exchanged(payload.reshape(devices, capacity, payload_width), EP)
    returned = back[:, :, :width].reshape(slot_total, width)
    dense_parts = back[:, :, width:].reshape(pairs, seq_count, dense_width)
    dense_parts = jnp.sum(dense_parts.astype(jnp.float32), axis=0)
    dense_hidden = jax.nn.silu(dense_parts[:, :head_size]) * dense_parts[:, head_size:]
    dense_terms = product_transposed(dense_hidden.astype(jnp.bfloat16), down_columns)
    side_total = (
        routes[0] * product(select_first, returned)
        + routes[1] * product(select_second, returned)
        + mix[:, None] * dense_terms
    )
    result = residual.astype(jnp.float32) + summed_over_heads(side_total.astype(jnp.bfloat16))
    return result.astype(jnp.bfloat16)


def solution(mesh):
    chips = mesh.shape["ep"] // 2
    finer = Mesh(mesh.devices.reshape(chips // 4, 4, 2, 4, 4), ("zh", "zl", "c", "y", "x"))
    in_specs = (
        P(EP, None),
        P(),
        P(EP, TP),
        P(EP, TP),
        P(EP, TP),
        P(None, TP),
        P(TP),
        P(EP, TP, None, None),
        P(EP, TP, None, None),
        P(EP, TP, None),
        P(EP),
        P(TP, EP),
        P(),
        P(EP, TP),
        P(EP, TP),
        P(TP, EP),
        P(),
        P(EP, None),
        P(EP),
        P(EP, None),
        P(EP, None, TP),
        P(EP, None, TP),
        P(EP, TP, None),
    )
    out_specs = P(EP, None)
    return jax.shard_map(layer, mesh=finer, in_specs=in_specs, out_specs=out_specs, check_vma=False)
```

```python
import math

import jax
import jax.numpy as jnp
from jax import lax
from jax.experimental import pallas as pl
from jax.experimental.pallas import tpu as pltpu
from jax.sharding import Mesh
from jax.sharding import PartitionSpec as P


EP = ("zh", "zl", "c")
Z = ("zh", "zl")
TP = ("y", "x")
EPSILON = 1e-06


def exchanged(pieces, axes):
    return lax.all_to_all(pieces, axes, split_axis=0, concat_axis=0, tiled=True)


def from_all(array, axis):
    return exchanged(jnp.broadcast_to(array, (lax.axis_size(axis), *array.shape)), axis)


def summed_at_once(array):
    return jnp.sum(from_all(array, TP).astype(jnp.float32), axis=0)


def summed_over_heads(array):
    rows = jnp.sum(from_all(array, "x").astype(jnp.float32), axis=0).astype(jnp.bfloat16)
    return jnp.sum(from_all(rows, "y").astype(jnp.float32), axis=0)


def in_order(own, theirs, place, dim):
    return jnp.where(
        place == 0,
        jnp.concatenate((own, theirs), axis=dim),
        jnp.concatenate((theirs, own), axis=dim),
    )


def product(left, right):
    return jnp.dot(left, right, preferred_element_type=jnp.float32)


def product_transposed(left, right):
    return lax.dot_general(
        left, right, (((1,), (1,)), ((), ())), preferred_element_type=jnp.float32
    )


def rms_scale(values, norm_gain):
    widened = values.astype(jnp.float32)
    return (
        widened
        * lax.rsqrt(jnp.mean(widened * widened, axis=-1, keepdims=True) + EPSILON)
        * norm_gain
    )


def first_payload(
    tokens_ref, gain_ref, out_ref, down_ref, query_ref, key_ref, value_ref, gate_ref, up_ref,
    forget_ref, bias_ref, ids_ref, pair_ref, group_ref,
    payload_ref, logits_ref, rows_ref, first_ref, second_ref, routes_ref,
):
    seq_count, _ = tokens_ref.shape
    chips, _, slab = payload_ref.shape
    half = seq_count // 2
    held = out_ref.shape[0] // 2
    for k, weight_ref in enumerate((query_ref, key_ref, value_ref, gate_ref, up_ref)):
        rows_ref[:, k * slab : (k + 1) * slab] = weight_ref[...]
    widened = tokens_ref[...].astype(jnp.float32)
    mean = jnp.mean(widened * widened, axis=-1, keepdims=True)
    normed = (widened * lax.rsqrt(mean + EPSILON) * gain_ref[...]).astype(jnp.bfloat16)
    forget = normed.astype(jnp.float32) * forget_ref[...].astype(jnp.float32)
    logits_ref[...] = jnp.sum(forget, axis=-1, keepdims=True) + bias_ref[...]
    for chip in range(chips):
        pair, side = divmod(chip, 2)
        for k in range(2):
            first = (2 * pair + k) * slab
            payload_ref[chip, k * half : (k + 1) * half, :] = normed[
                side * half : (side + 1) * half, first : first + slab
            ]
        columns = slice(side * held, (side + 1) * held)
        payload_ref[chip, seq_count : seq_count + held, :] = out_ref[columns, :]
        payload_ref[chip, seq_count + held :, :] = down_ref[columns, :]

    row = lax.broadcasted_iota(jnp.int32, (seq_count, seq_count), 0)
    place = lax.broadcasted_iota(jnp.int32, (seq_count, seq_count), 1)

    def column(values):
        return jnp.sum(jnp.where(row == place, values, 0.0), axis=1, keepdims=True)

    slot_total = first_ref.shape[1]
    devices = 2 * chips
    grid = lax.broadcasted_iota(jnp.int32, (seq_count, devices), 1).astype(jnp.float32)
    slots = lax.broadcasted_iota(jnp.int32, (seq_count, slot_total), 1).astype(jnp.float32)
    named = [column(ids_ref[k : k + 1, :].astype(jnp.float32)) for k in range(2)]
    hot = [(expert == grid).astype(jnp.float32) for expert in named]
    before = jnp.dot(
        (place < row).astype(jnp.float32), hot[0] + hot[1], preferred_element_type=jnp.float32
    )
    for k, select_ref in enumerate((first_ref, second_ref)):
        rank = jnp.sum(before * hot[k], axis=1, keepdims=True)
        target = named[k] * (slot_total // devices) + rank
        select_ref[...] = (target == slots).astype(jnp.float32).astype(jnp.bfloat16)
    odds = [column(pair_ref[k : k + 1, :]) for k in range(2)]
    group = column(group_ref[...])
    for k in range(2):
        routes_ref[k] = group * odds[k] / (odds[0] + odds[1])


def experts(
    rows_ref, dense_ref, gate_hbm, up_hbm, down_hbm, payload_ref,
    gate_ref, up_ref, down_ref, low_ref, high_ref, mixed_ref, sems,
):
    lanes, slots, _ = rows_ref.shape
    width, hidden_width = gate_ref.shape
    share = width // lanes
    slab = dense_ref.shape[0] // 2
    dense_width = hidden_width * 2
    first = dense_ref.shape[1] - dense_width
    copies = [
        pltpu.make_async_copy(source, target, sems.at[k])
        for k, (source, target) in enumerate(
            ((gate_hbm, gate_ref), (up_hbm, up_ref), (down_hbm, down_ref))
        )
    ]
    for copy in copies:
        copy.start()
    for lane in range(lanes):
        pieces = rows_ref[lane, :, share : share + slab]
        low = jnp.dot(pieces, dense_ref[:slab, first:], preferred_element_type=jnp.float32)
        high = jnp.dot(pieces, dense_ref[slab:, first:], preferred_element_type=jnp.float32)
        row, place = divmod(lane, 2)
        for part in range(2):
            span = slice(part * hidden_width, (part + 1) * hidden_width)
            low_ref[part] = low[:, span]
            high_ref[part] = high[:, span]
            mixed_ref[2 * place + part, pl.ds(row, slots // 2, stride=2), :] = (
                low_ref[part, pl.ds(0, slots // 2, stride=2), :]
                + high_ref[part, pl.ds(1, slots // 2, stride=2), :]
            )
    for part in range(mixed_ref.shape[0]):
        span = slice(width + part * hidden_width, width + (part + 1) * hidden_width)
        payload_ref[:, span] = mixed_ref[part].astype(jnp.bfloat16)
    copies[0].wait()
    copies[1].wait()
    gate_part = jnp.zeros((slots, hidden_width), jnp.float32)
    up_part = jnp.zeros((slots, hidden_width), jnp.float32)
    for lane in range(lanes):
        rows = rows_ref[lane, :, :share]
        span = slice(lane * share, (lane + 1) * share)
        gate_part += jnp.dot(rows, gate_ref[span, :], preferred_element_type=jnp.float32)
        up_part += jnp.dot(rows, up_ref[span, :], preferred_element_type=jnp.float32)
    hidden = (gate_part / (1.0 + jnp.exp(-gate_part)) * up_part).astype(jnp.bfloat16)
    copies[2].wait()
    payload_ref[:, :width] = jnp.dot(
        hidden, down_ref[...], preferred_element_type=jnp.float32
    ).astype(jnp.bfloat16)


def attend(queries, keys_new, values_new, key_cache, value_cache, gate_cache, lengths, log_forget):
    cache_span = key_cache.shape[2]
    score_scale = 1.0 / math.sqrt(key_cache.shape[3])
    positions = jnp.arange(cache_span, dtype=jnp.int32)
    live_mask = positions[None, :] < lengths[:, None]
    last_mask = positions[None, :] == lengths[:, None] - 1
    last_gate = jnp.sum(jnp.where(last_mask[:, None, :], gate_cache, 0.0), axis=-1)
    gate_now = last_gate + log_forget
    scores = (
        jnp.einsum("shd,shpd->shp", queries, key_cache, preferred_element_type=jnp.float32)
        * score_scale
    )
    scores = scores + gate_now[:, :, None] - gate_cache
    scores = jnp.where(live_mask[:, None, :], scores, -jnp.inf)
    own_score = (
        jnp.sum(queries.astype(jnp.float32) * keys_new.astype(jnp.float32), axis=-1) * score_scale
    )
    row_top = jnp.maximum(jnp.max(scores, axis=-1), own_score)
    raised = jnp.exp(scores - row_top[:, :, None])
    own_raised = jnp.exp(own_score - row_top)
    totals = jnp.sum(raised, axis=-1) + own_raised
    weights_low = (raised / totals[:, :, None]).astype(jnp.bfloat16)
    own_prob = (own_raised / totals).astype(jnp.bfloat16)
    attended = jnp.einsum(
        "shp,shpd->shd", weights_low, value_cache, preferred_element_type=jnp.float32
    )
    attended = attended + own_prob.astype(jnp.float32)[:, :, None] * values_new.astype(jnp.float32)
    return attended.astype(jnp.bfloat16)


def layer(
    tokens,
    attn_gain,
    query_weight,
    key_weight,
    value_weight,
    forget_weight,
    forget_bias,
    cache_keys,
    cache_values,
    cache_gates,
    lengths,
    output_weight,
    ffn_gain,
    dense_gate_proj,
    dense_up_proj,
    dense_down_proj,
    dense_mix,
    expert_ids,
    group_prob,
    pair_prob,
    expert_gate,
    expert_up,
    expert_down,
):
    seq_count, width = tokens.shape
    head_size = cache_keys.shape[3]
    chips = lax.axis_size(Z)
    quarters = lax.axis_size("zl")
    devices = lax.axis_size(EP)
    slab = width // chips
    core = lax.axis_index("c")
    side = lax.axis_index("zl") % 2
    pairs = chips // 2
    half = seq_count // 2

    held = output_weight.shape[1] // 2
    vmem = pl.BlockSpec(memory_space=pltpu.VMEM)
    capacity = 4 * seq_count // devices
    slot_total = devices * capacity
    payload, forget_logits, own_rows, *routing = pl.pallas_call(
        first_payload,
        out_shape=(
            jax.ShapeDtypeStruct((chips, seq_count + 2 * held, slab), jnp.bfloat16),
            jax.ShapeDtypeStruct((seq_count, 1), jnp.float32),
            pltpu.VMEM((query_weight.shape[0], 5 * slab), jnp.bfloat16),
            jax.ShapeDtypeStruct((seq_count, slot_total), jnp.bfloat16),
            jax.ShapeDtypeStruct((seq_count, slot_total), jnp.bfloat16),
            jax.ShapeDtypeStruct((2, seq_count, 1), jnp.float32),
        ),
        in_specs=(vmem,) * 14,
        out_specs=(vmem,) * 6,
        name="first_payload",
    )(
        tokens,
        attn_gain[None],
        output_weight.T,
        dense_down_proj.T,
        query_weight,
        key_weight,
        value_weight,
        dense_gate_proj,
        dense_up_proj,
        forget_weight.T,
        forget_bias[None],
        expert_ids.T,
        pair_prob.T,
        group_prob[None],
    )
    select_first, select_second, routes = routing
    received = exchanged(payload, Z)

    swap = [(0, 1), (1, 0)]
    neighbours = [(k, k ^ 1) for k in range(quarters)]
    their_rows = lax.ppermute(own_rows, "c", swap)
    chip_rows = in_order(own_rows, their_rows, core, 0)
    pair_rows = in_order(chip_rows, lax.ppermute(chip_rows, "zl", neighbours), side, 0)
    projection_width = 3 * head_size
    token_columns = received[:, :seq_count].reshape(chips, 2, half, slab)
    token_columns = token_columns.transpose(0, 2, 1, 3).reshape(chips * half, 2 * slab)

    halves = received[:, seq_count:].reshape(chips, 2, 1, held, slab)
    other_halves = lax.ppermute(halves, "zl", neighbours)
    both = in_order(halves, other_halves, side, 2)
    columns = in_order(both[:, None], lax.ppermute(both, "c", swap)[:, None], core, 1)
    output_columns = columns[:, :, 0].reshape(width, head_size)
    down_columns = columns[:, :, 1].reshape(width, head_size)

    shares = product(token_columns, pair_rows[:, :projection_width]).astype(jnp.bfloat16)
    shares = exchanged(shares.reshape(chips, half, projection_width), Z)
    shares = shares.reshape(pairs, seq_count, projection_width)
    projected = jnp.sum(shares.astype(jnp.float32), axis=0).astype(jnp.bfloat16)
    projected = projected.reshape(seq_count, 3, 1, head_size)
    log_forget = jax.nn.log_sigmoid(forget_logits)
    attended = attend(
        projected[:, 0],
        projected[:, 1],
        projected[:, 2],
        cache_keys,
        cache_values,
        cache_gates,
        lengths,
        log_forget,
    ).reshape(seq_count, head_size)
    head_terms = product_transposed(attended, output_columns).astype(jnp.bfloat16)
    lane = lax.axis_index("x")
    share = width // lax.axis_size("x")
    head_terms, selectors, routes, lane, share_start, mix_row = lax.optimization_barrier(
        (
            head_terms,
            (select_first, select_second),
            (routes[0], routes[1]),
            lane,
            lane * share,
            dense_mix.astype(jnp.float32),
        )
    )
    select_first, select_second = selectors
    residual = (tokens.astype(jnp.float32) + summed_over_heads(head_terms)).astype(jnp.bfloat16)
    ffn_in = rms_scale(residual, ffn_gain).astype(jnp.bfloat16)
    mix = jax.nn.sigmoid(jnp.sum(ffn_in.astype(jnp.float32) * mix_row, axis=-1))

    lanes = lax.axis_size("x")
    ffn_share = lax.dynamic_slice_in_dim(
        ffn_in, share_start, share, axis=1, allow_negative_indices=False
    )
    outbound = jnp.einsum(
        "sk,sd->kd", select_first + select_second, ffn_share, preferred_element_type=jnp.float32
    )
    outbound = outbound.astype(jnp.bfloat16).reshape(devices, capacity, share)
    few = seq_count // 4
    dense_pieces = ffn_in.reshape(4, few, pairs, 2, slab)
    dense_pieces = lax.dynamic_index_in_dim(
        dense_pieces, lane, axis=1, keepdims=False, allow_negative_indices=False
    )
    dense_pieces = dense_pieces.transpose(1, 0, 2, 3).reshape(devices, 2, slab)
    outbound, mix = lax.optimization_barrier(
        (jnp.concatenate((outbound, dense_pieces), axis=2), mix)
    )
    arrived = exchanged(outbound, EP)
    arrived = from_all(arrived, "x")
    dense_width = 2 * head_size
    payload_width = width + few // capacity * dense_width
    hbm = pl.BlockSpec(memory_space=pl.ANY)
    payload = pl.pallas_call(
        experts,
        out_shape=pltpu.VMEM((slot_total, payload_width), jnp.bfloat16),
        in_specs=(vmem, vmem, hbm, hbm, hbm),
        out_specs=vmem,
        scratch_shapes=(
            pltpu.VMEM(expert_gate.shape[1:], jnp.bfloat16),
            pltpu.VMEM(expert_up.shape[1:], jnp.bfloat16),
            pltpu.VMEM(expert_down.shape[1:], jnp.bfloat16),
            pltpu.VMEM((2, slot_total, head_size), jnp.float32),
            pltpu.VMEM((2, slot_total, head_size), jnp.float32),
            pltpu.VMEM(((payload_width - width) // head_size, slot_total, head_size), jnp.float32),
            pltpu.SemaphoreType.DMA((3,)),
        ),
        name="experts",
    )(
        pltpu.with_memory_space_constraint(
            arrived.reshape(lanes, slot_total, share + slab), pltpu.VMEM
        ),
        pair_rows,
        expert_gate[0],
        expert_up[0],
        expert_down[0],
    )
    back = exchanged(payload.reshape(devices, capacity, payload_width), EP)
    returned = back[:, :, :width].reshape(slot_total, width)
    dense_parts = back[:, :, width:].reshape(pairs, seq_count, dense_width)
    dense_parts = jnp.sum(dense_parts.astype(jnp.float32), axis=0)
    dense_hidden = jax.nn.silu(dense_parts[:, :head_size]) * dense_parts[:, head_size:]
    dense_terms = product_transposed(dense_hidden.astype(jnp.bfloat16), down_columns)
    side_total = (
        routes[0] * product(select_first, returned)
        + routes[1] * product(select_second, returned)
        + mix[:, None] * dense_terms
    )
    result = residual.astype(jnp.float32) + summed_at_once(side_total.astype(jnp.bfloat16))
    return result.astype(jnp.bfloat16)


def solution(mesh):
    chips = mesh.shape["ep"] // 2
    finer = Mesh(mesh.devices.reshape(chips // 4, 4, 2, 4, 4), ("zh", "zl", "c", "y", "x"))
    in_specs = (
        P(EP, None),
        P(),
        P(EP, TP),
        P(EP, TP),
        P(EP, TP),
        P(None, TP),
        P(TP),
        P(EP, TP, None, None),
        P(EP, TP, None, None),
        P(EP, TP, None),
        P(EP),
        P(TP, EP),
        P(),
        P(EP, TP),
        P(EP, TP),
        P(TP, EP),
        P(),
        P(EP, None),
        P(EP),
        P(EP, None),
        P(EP, None, TP),
        P(EP, None, TP),
        P(EP, TP, None),
    )
    out_specs = P(EP, None)
    return jax.shard_map(layer, mesh=finer, in_specs=in_specs, out_specs=out_specs, check_vma=False)
```

```python
import math

import jax
import jax.numpy as jnp
from jax import lax
from jax.experimental import pallas as pl
from jax.experimental.pallas import tpu as pltpu
from jax.sharding import Mesh
from jax.sharding import PartitionSpec as P


EP = ("zh", "zl", "c")
Z = ("zh", "zl")
TP = ("y", "x")
EPSILON = 1e-06


def exchanged(pieces, axes):
    return lax.all_to_all(pieces, axes, split_axis=0, concat_axis=0, tiled=True)


def from_all(array, axis):
    return exchanged(jnp.broadcast_to(array, (lax.axis_size(axis), *array.shape)), axis)


def summed_over_heads(array):
    rows = jnp.sum(from_all(array, "x").astype(jnp.float32), axis=0).astype(jnp.bfloat16)
    return jnp.sum(from_all(rows, "y").astype(jnp.float32), axis=0)


def in_order(own, theirs, place, dim):
    return jnp.where(
        place == 0,
        jnp.concatenate((own, theirs), axis=dim),
        jnp.concatenate((theirs, own), axis=dim),
    )


def product(left, right):
    return jnp.dot(left, right, preferred_element_type=jnp.float32)


def product_transposed(left, right):
    return lax.dot_general(
        left, right, (((1,), (1,)), ((), ())), preferred_element_type=jnp.float32
    )


def rms_scale(values, norm_gain):
    widened = values.astype(jnp.float32)
    return (
        widened
        * lax.rsqrt(jnp.mean(widened * widened, axis=-1, keepdims=True) + EPSILON)
        * norm_gain
    )


def first_payload(
    tokens_ref, gain_ref, out_ref, down_ref, query_ref, key_ref, value_ref, gate_ref, up_ref,
    forget_ref, bias_ref, ids_ref, pair_ref, group_ref,
    payload_ref, logits_ref, rows_ref, first_ref, second_ref, routes_ref,
):
    seq_count, _ = tokens_ref.shape
    chips, _, slab = payload_ref.shape
    half = seq_count // 2
    held = out_ref.shape[0] // 2
    for k, weight_ref in enumerate((query_ref, key_ref, value_ref, gate_ref, up_ref)):
        rows_ref[:, k * slab : (k + 1) * slab] = weight_ref[...]
    widened = tokens_ref[...].astype(jnp.float32)
    mean = jnp.mean(widened * widened, axis=-1, keepdims=True)
    normed = (widened * lax.rsqrt(mean + EPSILON) * gain_ref[...]).astype(jnp.bfloat16)
    forget = normed.astype(jnp.float32) * forget_ref[...].astype(jnp.float32)
    logits_ref[...] = jnp.sum(forget, axis=-1, keepdims=True) + bias_ref[...]
    for chip in range(chips):
        pair, side = divmod(chip, 2)
        for k in range(2):
            first = (2 * pair + k) * slab
            payload_ref[chip, k * half : (k + 1) * half, :] = normed[
                side * half : (side + 1) * half, first : first + slab
            ]
        columns = slice(side * held, (side + 1) * held)
        payload_ref[chip, seq_count : seq_count + held, :] = out_ref[columns, :]
        payload_ref[chip, seq_count + held :, :] = down_ref[columns, :]

    row = lax.broadcasted_iota(jnp.int32, (seq_count, seq_count), 0)
    place = lax.broadcasted_iota(jnp.int32, (seq_count, seq_count), 1)

    def column(values):
        return jnp.sum(jnp.where(row == place, values, 0.0), axis=1, keepdims=True)

    slot_total = first_ref.shape[1]
    devices = 2 * chips
    grid = lax.broadcasted_iota(jnp.int32, (seq_count, devices), 1).astype(jnp.float32)
    slots = lax.broadcasted_iota(jnp.int32, (seq_count, slot_total), 1).astype(jnp.float32)
    named = [column(ids_ref[k : k + 1, :].astype(jnp.float32)) for k in range(2)]
    hot = [(expert == grid).astype(jnp.float32) for expert in named]
    before = jnp.dot(
        (place < row).astype(jnp.float32), hot[0] + hot[1], preferred_element_type=jnp.float32
    )
    for k, select_ref in enumerate((first_ref, second_ref)):
        rank = jnp.sum(before * hot[k], axis=1, keepdims=True)
        target = named[k] * (slot_total // devices) + rank
        select_ref[...] = (target == slots).astype(jnp.float32).astype(jnp.bfloat16)
    odds = [column(pair_ref[k : k + 1, :]) for k in range(2)]
    group = column(group_ref[...])
    for k in range(2):
        routes_ref[k] = group * odds[k] / (odds[0] + odds[1])


def experts(
    rows_ref, dense_ref, gate_hbm, up_hbm, down_hbm, payload_ref,
    gate_ref, up_ref, down_ref, low_ref, high_ref, mixed_ref, sems,
):
    lanes, slots, _ = rows_ref.shape
    width, hidden_width = gate_ref.shape
    share = width // lanes
    slab = dense_ref.shape[0] // 2
    dense_width = hidden_width * 2
    first = dense_ref.shape[1] - dense_width
    copies = [
        pltpu.make_async_copy(source, target, sems.at[k])
        for k, (source, target) in enumerate(
            ((gate_hbm, gate_ref), (up_hbm, up_ref), (down_hbm, down_ref))
        )
    ]
    for copy in copies:
        copy.start()
    for lane in range(lanes):
        pieces = rows_ref[lane, :, share : share + slab]
        low = jnp.dot(pieces, dense_ref[:slab, first:], preferred_element_type=jnp.float32)
        high = jnp.dot(pieces, dense_ref[slab:, first:], preferred_element_type=jnp.float32)
        row, place = divmod(lane, 2)
        for part in range(2):
            span = slice(part * hidden_width, (part + 1) * hidden_width)
            low_ref[part] = low[:, span]
            high_ref[part] = high[:, span]
            mixed_ref[2 * place + part, pl.ds(row, slots // 2, stride=2), :] = (
                low_ref[part, pl.ds(0, slots // 2, stride=2), :]
                + high_ref[part, pl.ds(1, slots // 2, stride=2), :]
            )
    for part in range(mixed_ref.shape[0]):
        span = slice(width + part * hidden_width, width + (part + 1) * hidden_width)
        payload_ref[:, span] = mixed_ref[part].astype(jnp.bfloat16)
    copies[0].wait()
    copies[1].wait()
    gate_part = jnp.zeros((slots, hidden_width), jnp.float32)
    up_part = jnp.zeros((slots, hidden_width), jnp.float32)
    for lane in range(lanes):
        rows = rows_ref[lane, :, :share]
        span = slice(lane * share, (lane + 1) * share)
        gate_part += jnp.dot(rows, gate_ref[span, :], preferred_element_type=jnp.float32)
        up_part += jnp.dot(rows, up_ref[span, :], preferred_element_type=jnp.float32)
    hidden = (gate_part / (1.0 + jnp.exp(-gate_part)) * up_part).astype(jnp.bfloat16)
    copies[2].wait()
    payload_ref[:, :width] = jnp.dot(
        hidden, down_ref[...], preferred_element_type=jnp.float32
    ).astype(jnp.bfloat16)


def attend(queries, keys_new, values_new, key_cache, value_cache, gate_cache, lengths, log_forget):
    cache_span = key_cache.shape[2]
    score_scale = 1.0 / math.sqrt(key_cache.shape[3])
    positions = jnp.arange(cache_span, dtype=jnp.int32)
    live_mask = positions[None, :] < lengths[:, None]
    last_mask = positions[None, :] == lengths[:, None] - 1
    last_gate = jnp.sum(jnp.where(last_mask[:, None, :], gate_cache, 0.0), axis=-1)
    gate_now = last_gate + log_forget
    scores = (
        jnp.einsum("shd,shpd->shp", queries, key_cache, preferred_element_type=jnp.float32)
        * score_scale
    )
    scores = scores + gate_now[:, :, None] - gate_cache
    scores = jnp.where(live_mask[:, None, :], scores, -jnp.inf)
    own_score = (
        jnp.sum(queries.astype(jnp.float32) * keys_new.astype(jnp.float32), axis=-1) * score_scale
    )
    row_top = jnp.maximum(jnp.max(scores, axis=-1), own_score)
    raised = jnp.exp(scores - row_top[:, :, None])
    own_raised = jnp.exp(own_score - row_top)
    totals = jnp.sum(raised, axis=-1) + own_raised
    weights_low = (raised / totals[:, :, None]).astype(jnp.bfloat16)
    own_prob = (own_raised / totals).astype(jnp.bfloat16)
    attended = jnp.einsum(
        "shp,shpd->shd", weights_low, value_cache, preferred_element_type=jnp.float32
    )
    attended = attended + own_prob.astype(jnp.float32)[:, :, None] * values_new.astype(jnp.float32)
    return attended.astype(jnp.bfloat16)


def layer(
    tokens,
    attn_gain,
    query_weight,
    key_weight,
    value_weight,
    forget_weight,
    forget_bias,
    cache_keys,
    cache_values,
    cache_gates,
    lengths,
    output_weight,
    ffn_gain,
    dense_gate_proj,
    dense_up_proj,
    dense_down_proj,
    dense_mix,
    expert_ids,
    group_prob,
    pair_prob,
    expert_gate,
    expert_up,
    expert_down,
):
    seq_count, width = tokens.shape
    head_size = cache_keys.shape[3]
    chips = lax.axis_size(Z)
    quarters = lax.axis_size("zl")
    devices = lax.axis_size(EP)
    slab = width // chips
    core = lax.axis_index("c")
    side = lax.axis_index("zl") % 2
    pairs = chips // 2
    half = seq_count // 2

    held = output_weight.shape[1] // 2
    vmem = pl.BlockSpec(memory_space=pltpu.VMEM)
    capacity = 4 * seq_count // devices
    slot_total = devices * capacity
    payload, forget_logits, own_rows, *routing = pl.pallas_call(
        first_payload,
        out_shape=(
            jax.ShapeDtypeStruct((chips, seq_count + 2 * held, slab), jnp.bfloat16),
            jax.ShapeDtypeStruct((seq_count, 1), jnp.float32),
            pltpu.VMEM((query_weight.shape[0], 5 * slab), jnp.bfloat16),
            jax.ShapeDtypeStruct((seq_count, slot_total), jnp.bfloat16),
            jax.ShapeDtypeStruct((seq_count, slot_total), jnp.bfloat16),
            jax.ShapeDtypeStruct((2, seq_count, 1), jnp.float32),
        ),
        in_specs=(vmem,) * 14,
        out_specs=(vmem,) * 6,
        name="first_payload",
    )(
        tokens,
        attn_gain[None],
        output_weight.T,
        dense_down_proj.T,
        query_weight,
        key_weight,
        value_weight,
        dense_gate_proj,
        dense_up_proj,
        forget_weight.T,
        forget_bias[None],
        expert_ids.T,
        pair_prob.T,
        group_prob[None],
    )
    select_first, select_second, routes = routing
    received = exchanged(payload, Z)

    swap = [(0, 1), (1, 0)]
    neighbours = [(k, k ^ 1) for k in range(quarters)]
    their_rows = lax.ppermute(own_rows, "c", swap)
    chip_rows = in_order(own_rows, their_rows, core, 0)
    pair_rows = in_order(chip_rows, lax.ppermute(chip_rows, "zl", neighbours), side, 0)
    projection_width = 3 * head_size
    token_columns = received[:, :seq_count].reshape(chips, 2, half, slab)
    token_columns = token_columns.transpose(0, 2, 1, 3).reshape(chips * half, 2 * slab)

    halves = received[:, seq_count:].reshape(chips, 2, 1, held, slab)
    other_halves = lax.ppermute(halves, "zl", neighbours)
    their_halves = lax.ppermute(halves, "c", swap)
    their_others = lax.ppermute(other_halves, "c", swap)
    columns = in_order(
        in_order(halves, other_halves, side, 2)[:, None],
        in_order(their_halves, their_others, side, 2)[:, None],
        core,
        1,
    )
    output_columns = columns[:, :, 0].reshape(width, head_size)
    down_columns = columns[:, :, 1].reshape(width, head_size)

    shares = product(token_columns, pair_rows[:, :projection_width]).astype(jnp.bfloat16)
    shares = exchanged(shares.reshape(chips, half, projection_width), Z)
    shares = shares.reshape(pairs, seq_count, projection_width)
    projected = jnp.sum(shares.astype(jnp.float32), axis=0).astype(jnp.bfloat16)
    projected = projected.reshape(seq_count, 3, 1, head_size)
    log_forget = jax.nn.log_sigmoid(forget_logits)
    attended = attend(
        projected[:, 0],
        projected[:, 1],
        projected[:, 2],
        cache_keys,
        cache_values,
        cache_gates,
        lengths,
        log_forget,
    ).reshape(seq_count, head_size)
    head_terms = product_transposed(attended, output_columns).astype(jnp.bfloat16)
    lane = lax.axis_index("x")
    share = width // lax.axis_size("x")
    head_terms, selectors, routes, lane, share_start, mix_row = lax.optimization_barrier(
        (
            head_terms,
            (select_first, select_second),
            (routes[0], routes[1]),
            lane,
            lane * share,
            dense_mix.astype(jnp.float32),
        )
    )
    select_first, select_second = selectors
    residual = (tokens.astype(jnp.float32) + summed_over_heads(head_terms)).astype(jnp.bfloat16)
    ffn_in = rms_scale(residual, ffn_gain).astype(jnp.bfloat16)
    mix = jax.nn.sigmoid(jnp.sum(ffn_in.astype(jnp.float32) * mix_row, axis=-1))

    lanes = lax.axis_size("x")
    ffn_share = lax.dynamic_slice_in_dim(
        ffn_in, share_start, share, axis=1, allow_negative_indices=False
    )
    outbound = jnp.einsum(
        "sk,sd->kd", select_first + select_second, ffn_share, preferred_element_type=jnp.float32
    )
    outbound = outbound.astype(jnp.bfloat16).reshape(devices, capacity, share)
    few = seq_count // 4
    dense_pieces = ffn_in.reshape(4, few, pairs, 2, slab)
    dense_pieces = lax.dynamic_index_in_dim(
        dense_pieces, lane, axis=1, keepdims=False, allow_negative_indices=False
    )
    dense_pieces = dense_pieces.transpose(1, 0, 2, 3).reshape(devices, 2, slab)
    outbound, mix = lax.optimization_barrier(
        (jnp.concatenate((outbound, dense_pieces), axis=2), mix)
    )
    arrived = exchanged(outbound, EP)
    arrived = from_all(arrived, "x")
    dense_width = 2 * head_size
    payload_width = width + few // capacity * dense_width
    hbm = pl.BlockSpec(memory_space=pl.ANY)
    payload = pl.pallas_call(
        experts,
        out_shape=pltpu.VMEM((slot_total, payload_width), jnp.bfloat16),
        in_specs=(vmem, vmem, hbm, hbm, hbm),
        out_specs=vmem,
        scratch_shapes=(
            pltpu.VMEM(expert_gate.shape[1:], jnp.bfloat16),
            pltpu.VMEM(expert_up.shape[1:], jnp.bfloat16),
            pltpu.VMEM(expert_down.shape[1:], jnp.bfloat16),
            pltpu.VMEM((2, slot_total, head_size), jnp.float32),
            pltpu.VMEM((2, slot_total, head_size), jnp.float32),
            pltpu.VMEM(((payload_width - width) // head_size, slot_total, head_size), jnp.float32),
            pltpu.SemaphoreType.DMA((3,)),
        ),
        name="experts",
    )(
        pltpu.with_memory_space_constraint(
            arrived.reshape(lanes, slot_total, share + slab), pltpu.VMEM
        ),
        pair_rows,
        expert_gate[0],
        expert_up[0],
        expert_down[0],
    )
    back = exchanged(payload.reshape(devices, capacity, payload_width), EP)
    returned = back[:, :, :width].reshape(slot_total, width)
    dense_parts = back[:, :, width:].reshape(pairs, seq_count, dense_width)
    dense_parts = jnp.sum(dense_parts.astype(jnp.float32), axis=0)
    dense_hidden = jax.nn.silu(dense_parts[:, :head_size]) * dense_parts[:, head_size:]
    dense_terms = product_transposed(dense_hidden.astype(jnp.bfloat16), down_columns)
    side_total = (
        routes[0] * product(select_first, returned)
        + routes[1] * product(select_second, returned)
        + mix[:, None] * dense_terms
    )
    result = residual.astype(jnp.float32) + summed_over_heads(side_total.astype(jnp.bfloat16))
    return result.astype(jnp.bfloat16)


def solution(mesh):
    chips = mesh.shape["ep"] // 2
    finer = Mesh(mesh.devices.reshape(chips // 4, 4, 2, 4, 4), ("zh", "zl", "c", "y", "x"))
    in_specs = (
        P(EP, None),
        P(),
        P(EP, TP),
        P(EP, TP),
        P(EP, TP),
        P(None, TP),
        P(TP),
        P(EP, TP, None, None),
        P(EP, TP, None, None),
        P(EP, TP, None),
        P(EP),
        P(TP, EP),
        P(),
        P(EP, TP),
        P(EP, TP),
        P(TP, EP),
        P(),
        P(EP, None),
        P(EP),
        P(EP, None),
        P(EP, None, TP),
        P(EP, None, TP),
        P(EP, TP, None),
    )
    out_specs = P(EP, None)
    return jax.shard_map(layer, mesh=finer, in_specs=in_specs, out_specs=out_specs, check_vma=False)
```

```python
import math

import jax
import jax.numpy as jnp
from jax import lax
from jax.experimental import pallas as pl
from jax.experimental.pallas import tpu as pltpu
from jax.sharding import Mesh
from jax.sharding import PartitionSpec as P


EP = ("zh", "zl", "c")
Z = ("zh", "zl")
TP = ("y", "x")
EPSILON = 1e-06


def exchanged(pieces, axes):
    return lax.all_to_all(pieces, axes, split_axis=0, concat_axis=0, tiled=True)


def from_all(array, axis):
    return exchanged(jnp.broadcast_to(array, (lax.axis_size(axis), *array.shape)), axis)


def summed_over_heads(array):
    rows = jnp.sum(from_all(array, "x").astype(jnp.float32), axis=0).astype(jnp.bfloat16)
    return jnp.sum(from_all(rows, "y").astype(jnp.float32), axis=0)


def in_order(own, theirs, place, dim):
    return jnp.where(
        place == 0,
        jnp.concatenate((own, theirs), axis=dim),
        jnp.concatenate((theirs, own), axis=dim),
    )


def product(left, right):
    return jnp.dot(left, right, preferred_element_type=jnp.float32)


def product_transposed(left, right):
    return lax.dot_general(
        left, right, (((1,), (1,)), ((), ())), preferred_element_type=jnp.float32
    )


def rms_scale(values, norm_gain):
    widened = values.astype(jnp.float32)
    return (
        widened
        * lax.rsqrt(jnp.mean(widened * widened, axis=-1, keepdims=True) + EPSILON)
        * norm_gain
    )


def first_payload(
    tokens_ref, gain_ref, out_ref, down_ref, query_ref, key_ref, value_ref, gate_ref, up_ref,
    forget_ref, bias_ref, ids_ref, pair_ref, group_ref,
    payload_ref, logits_ref, rows_ref, first_ref, second_ref, routes_ref,
):
    seq_count, _ = tokens_ref.shape
    chips, _, slab = payload_ref.shape
    half = seq_count // 2
    held = out_ref.shape[0] // 2
    for k, weight_ref in enumerate((query_ref, key_ref, value_ref, gate_ref, up_ref)):
        rows_ref[:, k * slab : (k + 1) * slab] = weight_ref[...]
    widened = tokens_ref[...].astype(jnp.float32)
    mean = jnp.mean(widened * widened, axis=-1, keepdims=True)
    normed = (widened * lax.rsqrt(mean + EPSILON) * gain_ref[...]).astype(jnp.bfloat16)
    forget = normed.astype(jnp.float32) * forget_ref[...].astype(jnp.float32)
    logits_ref[...] = jnp.sum(forget, axis=-1, keepdims=True) + bias_ref[...]
    for chip in range(chips):
        pair, side = divmod(chip, 2)
        for k in range(2):
            first = (2 * pair + k) * slab
            payload_ref[chip, k * half : (k + 1) * half, :] = normed[
                side * half : (side + 1) * half, first : first + slab
            ]
        columns = slice(side * held, (side + 1) * held)
        payload_ref[chip, seq_count : seq_count + held, :] = out_ref[columns, :]
        payload_ref[chip, seq_count + held :, :] = down_ref[columns, :]

    row = lax.broadcasted_iota(jnp.int32, (seq_count, seq_count), 0)
    place = lax.broadcasted_iota(jnp.int32, (seq_count, seq_count), 1)

    def column(values):
        return jnp.sum(jnp.where(row == place, values, 0.0), axis=1, keepdims=True)

    slot_total = first_ref.shape[1]
    devices = 2 * chips
    grid = lax.broadcasted_iota(jnp.int32, (seq_count, devices), 1).astype(jnp.float32)
    slots = lax.broadcasted_iota(jnp.int32, (seq_count, slot_total), 1).astype(jnp.float32)
    named = [column(ids_ref[k : k + 1, :].astype(jnp.float32)) for k in range(2)]
    hot = [(expert == grid).astype(jnp.float32) for expert in named]
    before = jnp.dot(
        (place < row).astype(jnp.float32), hot[0] + hot[1], preferred_element_type=jnp.float32
    )
    for k, select_ref in enumerate((first_ref, second_ref)):
        rank = jnp.sum(before * hot[k], axis=1, keepdims=True)
        target = named[k] * (slot_total // devices) + rank
        select_ref[...] = (target == slots).astype(jnp.float32).astype(jnp.bfloat16)
    odds = [column(pair_ref[k : k + 1, :]) for k in range(2)]
    group = column(group_ref[...])
    for k in range(2):
        routes_ref[k] = group * odds[k] / (odds[0] + odds[1])


def experts(
    rows_ref, dense_ref, gate_hbm, up_hbm, down_hbm, payload_ref,
    gate_ref, up_ref, down_ref, low_ref, high_ref, mixed_ref, sems,
):
    lanes, slots, _ = rows_ref.shape
    width, hidden_width = gate_ref.shape
    share = width // lanes
    slab = dense_ref.shape[0] // 2
    dense_width = hidden_width * 2
    first = dense_ref.shape[1] - dense_width
    copies = [
        pltpu.make_async_copy(source, target, sems.at[k])
        for k, (source, target) in enumerate(
            ((gate_hbm, gate_ref), (up_hbm, up_ref), (down_hbm, down_ref))
        )
    ]
    for copy in copies:
        copy.start()
    for lane in range(lanes):
        pieces = rows_ref[lane, :, share : share + slab]
        low = jnp.dot(pieces, dense_ref[:slab, first:], preferred_element_type=jnp.float32)
        high = jnp.dot(pieces, dense_ref[slab:, first:], preferred_element_type=jnp.float32)
        row, place = divmod(lane, 2)
        for part in range(2):
            span = slice(part * hidden_width, (part + 1) * hidden_width)
            low_ref[part] = low[:, span]
            high_ref[part] = high[:, span]
            mixed_ref[2 * place + part, pl.ds(row, slots // 2, stride=2), :] = (
                low_ref[part, pl.ds(0, slots // 2, stride=2), :]
                + high_ref[part, pl.ds(1, slots // 2, stride=2), :]
            )
    for part in range(mixed_ref.shape[0]):
        span = slice(width + part * hidden_width, width + (part + 1) * hidden_width)
        payload_ref[:, span] = mixed_ref[part].astype(jnp.bfloat16)
    copies[0].wait()
    copies[1].wait()
    gate_part = jnp.zeros((slots, hidden_width), jnp.float32)
    up_part = jnp.zeros((slots, hidden_width), jnp.float32)
    for lane in range(lanes):
        rows = rows_ref[lane, :, :share]
        span = slice(lane * share, (lane + 1) * share)
        gate_part += jnp.dot(rows, gate_ref[span, :], preferred_element_type=jnp.float32)
        up_part += jnp.dot(rows, up_ref[span, :], preferred_element_type=jnp.float32)
    hidden = (gate_part / (1.0 + jnp.exp(-gate_part)) * up_part).astype(jnp.bfloat16)
    copies[2].wait()
    payload_ref[:, :width] = jnp.dot(
        hidden, down_ref[...], preferred_element_type=jnp.float32
    ).astype(jnp.bfloat16)


def attend(queries, keys_new, values_new, key_cache, value_cache, gate_cache, lengths, log_forget):
    cache_span = key_cache.shape[2]
    score_scale = 1.0 / math.sqrt(key_cache.shape[3])
    positions = jnp.arange(cache_span, dtype=jnp.int32)
    live_mask = positions[None, :] < lengths[:, None]
    last_mask = positions[None, :] == lengths[:, None] - 1
    last_gate = jnp.sum(jnp.where(last_mask[:, None, :], gate_cache, 0.0), axis=-1)
    gate_now = last_gate + log_forget
    scores = (
        jnp.einsum("shd,shpd->shp", queries, key_cache, preferred_element_type=jnp.float32)
        * score_scale
    )
    scores = scores + gate_now[:, :, None] - gate_cache
    scores = jnp.where(live_mask[:, None, :], scores, -jnp.inf)
    own_score = (
        jnp.sum(queries.astype(jnp.float32) * keys_new.astype(jnp.float32), axis=-1) * score_scale
    )
    row_top = jnp.maximum(jnp.max(scores, axis=-1), own_score)
    raised = jnp.exp(scores - row_top[:, :, None])
    own_raised = jnp.exp(own_score - row_top)
    totals = jnp.sum(raised, axis=-1) + own_raised
    weights_low = (raised / totals[:, :, None]).astype(jnp.bfloat16)
    own_prob = (own_raised / totals).astype(jnp.bfloat16)
    attended = jnp.einsum(
        "shp,shpd->shd", weights_low, value_cache, preferred_element_type=jnp.float32
    )
    attended = attended + own_prob.astype(jnp.float32)[:, :, None] * values_new.astype(jnp.float32)
    return attended.astype(jnp.bfloat16)


def layer(
    tokens,
    attn_gain,
    query_weight,
    key_weight,
    value_weight,
    forget_weight,
    forget_bias,
    cache_keys,
    cache_values,
    cache_gates,
    lengths,
    output_weight,
    ffn_gain,
    dense_gate_proj,
    dense_up_proj,
    dense_down_proj,
    dense_mix,
    expert_ids,
    group_prob,
    pair_prob,
    expert_gate,
    expert_up,
    expert_down,
):
    seq_count, width = tokens.shape
    head_size = cache_keys.shape[3]
    chips = lax.axis_size(Z)
    quarters = lax.axis_size("zl")
    devices = lax.axis_size(EP)
    slab = width // chips
    core = lax.axis_index("c")
    side = lax.axis_index("zl") % 2
    pairs = chips // 2
    half = seq_count // 2

    held = output_weight.shape[1] // 2
    vmem = pl.BlockSpec(memory_space=pltpu.VMEM)
    capacity = 4 * seq_count // devices
    slot_total = devices * capacity
    payload, forget_logits, own_rows, *routing = pl.pallas_call(
        first_payload,
        out_shape=(
            jax.ShapeDtypeStruct((chips, seq_count + 2 * held, slab), jnp.bfloat16),
            jax.ShapeDtypeStruct((seq_count, 1), jnp.float32),
            pltpu.VMEM((query_weight.shape[0], 5 * slab), jnp.bfloat16),
            jax.ShapeDtypeStruct((seq_count, slot_total), jnp.bfloat16),
            jax.ShapeDtypeStruct((seq_count, slot_total), jnp.bfloat16),
            jax.ShapeDtypeStruct((2, seq_count, 1), jnp.float32),
        ),
        in_specs=(vmem,) * 14,
        out_specs=(vmem,) * 6,
        name="first_payload",
    )(
        tokens,
        attn_gain[None],
        output_weight.T,
        dense_down_proj.T,
        query_weight,
        key_weight,
        value_weight,
        dense_gate_proj,
        dense_up_proj,
        forget_weight.T,
        forget_bias[None],
        expert_ids.T,
        pair_prob.T,
        group_prob[None],
    )
    select_first, select_second, routes = routing
    received = exchanged(payload, Z)

    swap = [(0, 1), (1, 0)]
    neighbours = [(k, k ^ 1) for k in range(quarters)]
    neighbour_rows = lax.ppermute(own_rows, "zl", neighbours)
    pair_rows = in_order(own_rows[None, None], neighbour_rows[None, None], side, 0)
    pair_rows = in_order(pair_rows, lax.ppermute(pair_rows, "c", swap), core, 1)
    pair_rows = pair_rows.reshape(4 * own_rows.shape[0], own_rows.shape[1])
    projection_width = 3 * head_size
    token_columns = received[:, :seq_count].reshape(chips, 2, half, slab)
    token_columns = token_columns.transpose(0, 2, 1, 3).reshape(chips * half, 2 * slab)

    halves = received[:, seq_count:].reshape(chips, 2, 1, held, slab)
    other_halves = lax.ppermute(halves, "zl", neighbours)
    their_halves = lax.ppermute(halves, "c", swap)
    their_others = lax.ppermute(other_halves, "c", swap)
    columns = in_order(
        in_order(halves, other_halves, side, 2)[:, None],
        in_order(their_halves, their_others, side, 2)[:, None],
        core,
        1,
    )
    output_columns = columns[:, :, 0].reshape(width, head_size)
    down_columns = columns[:, :, 1].reshape(width, head_size)

    shares = product(token_columns, pair_rows[:, :projection_width]).astype(jnp.bfloat16)
    shares = exchanged(shares.reshape(chips, half, projection_width), Z)
    shares = shares.reshape(pairs, seq_count, projection_width)
    projected = jnp.sum(shares.astype(jnp.float32), axis=0).astype(jnp.bfloat16)
    projected = projected.reshape(seq_count, 3, 1, head_size)
    log_forget = jax.nn.log_sigmoid(forget_logits)
    attended = attend(
        projected[:, 0],
        projected[:, 1],
        projected[:, 2],
        cache_keys,
        cache_values,
        cache_gates,
        lengths,
        log_forget,
    ).reshape(seq_count, head_size)
    head_terms = product_transposed(attended, output_columns).astype(jnp.bfloat16)
    lane = lax.axis_index("x")
    share = width // lax.axis_size("x")
    head_terms, selectors, routes, lane, share_start, mix_row = lax.optimization_barrier(
        (
            head_terms,
            (select_first, select_second),
            (routes[0], routes[1]),
            lane,
            lane * share,
            dense_mix.astype(jnp.float32),
        )
    )
    select_first, select_second = selectors
    residual = (tokens.astype(jnp.float32) + summed_over_heads(head_terms)).astype(jnp.bfloat16)
    ffn_in = rms_scale(residual, ffn_gain).astype(jnp.bfloat16)
    mix = jax.nn.sigmoid(jnp.sum(ffn_in.astype(jnp.float32) * mix_row, axis=-1))

    lanes = lax.axis_size("x")
    ffn_share = lax.dynamic_slice_in_dim(
        ffn_in, share_start, share, axis=1, allow_negative_indices=False
    )
    outbound = jnp.einsum(
        "sk,sd->kd", select_first + select_second, ffn_share, preferred_element_type=jnp.float32
    )
    outbound = outbound.astype(jnp.bfloat16).reshape(devices, capacity, share)
    few = seq_count // 4
    dense_pieces = ffn_in.reshape(4, few, pairs, 2, slab)
    dense_pieces = lax.dynamic_index_in_dim(
        dense_pieces, lane, axis=1, keepdims=False, allow_negative_indices=False
    )
    dense_pieces = dense_pieces.transpose(1, 0, 2, 3).reshape(devices, 2, slab)
    outbound, mix = lax.optimization_barrier(
        (jnp.concatenate((outbound, dense_pieces), axis=2), mix)
    )
    arrived = exchanged(outbound, EP)
    arrived = from_all(arrived, "x")
    dense_width = 2 * head_size
    payload_width = width + few // capacity * dense_width
    hbm = pl.BlockSpec(memory_space=pl.ANY)
    payload = pl.pallas_call(
        experts,
        out_shape=pltpu.VMEM((slot_total, payload_width), jnp.bfloat16),
        in_specs=(vmem, vmem, hbm, hbm, hbm),
        out_specs=vmem,
        scratch_shapes=(
            pltpu.VMEM(expert_gate.shape[1:], jnp.bfloat16),
            pltpu.VMEM(expert_up.shape[1:], jnp.bfloat16),
            pltpu.VMEM(expert_down.shape[1:], jnp.bfloat16),
            pltpu.VMEM((2, slot_total, head_size), jnp.float32),
            pltpu.VMEM((2, slot_total, head_size), jnp.float32),
            pltpu.VMEM(((payload_width - width) // head_size, slot_total, head_size), jnp.float32),
            pltpu.SemaphoreType.DMA((3,)),
        ),
        name="experts",
    )(
        pltpu.with_memory_space_constraint(
            arrived.reshape(lanes, slot_total, share + slab), pltpu.VMEM
        ),
        pair_rows,
        expert_gate[0],
        expert_up[0],
        expert_down[0],
    )
    back = exchanged(payload.reshape(devices, capacity, payload_width), EP)
    returned = back[:, :, :width].reshape(slot_total, width)
    dense_parts = back[:, :, width:].reshape(pairs, seq_count, dense_width)
    dense_parts = jnp.sum(dense_parts.astype(jnp.float32), axis=0)
    dense_hidden = jax.nn.silu(dense_parts[:, :head_size]) * dense_parts[:, head_size:]
    dense_terms = product_transposed(dense_hidden.astype(jnp.bfloat16), down_columns)
    side_total = (
        routes[0] * product(select_first, returned)
        + routes[1] * product(select_second, returned)
        + mix[:, None] * dense_terms
    )
    result = residual.astype(jnp.float32) + summed_over_heads(side_total.astype(jnp.bfloat16))
    return result.astype(jnp.bfloat16)


def solution(mesh):
    chips = mesh.shape["ep"] // 2
    finer = Mesh(mesh.devices.reshape(chips // 4, 4, 2, 4, 4), ("zh", "zl", "c", "y", "x"))
    in_specs = (
        P(EP, None),
        P(),
        P(EP, TP),
        P(EP, TP),
        P(EP, TP),
        P(None, TP),
        P(TP),
        P(EP, TP, None, None),
        P(EP, TP, None, None),
        P(EP, TP, None),
        P(EP),
        P(TP, EP),
        P(),
        P(EP, TP),
        P(EP, TP),
        P(TP, EP),
        P(),
        P(EP, None),
        P(EP),
        P(EP, None),
        P(EP, None, TP),
        P(EP, None, TP),
        P(EP, TP, None),
    )
    out_specs = P(EP, None)
    return jax.shard_map(layer, mesh=finer, in_specs=in_specs, out_specs=out_specs, check_vma=False)
```
